32 devices in a mesh: sp: 8 (over z, x), tp: 4 (over y, core).
Axes of the slice: x: 2, y: 2, z: 4, core: 2. Of those that a mesh axis runs over, the one named last changes fastest.
Arguments:
- tokens: bfloat16 [8, 80, 4096], P(None, 'sp', 'tp'), may hold values from -6 to 6
- latent_down_weight: bfloat16 [4096, 512], replicated, may hold values from -0.09375 to 0.09375
- w_rope_key: bfloat16 [4096, 64], replicated, may hold values from -0.09375 to 0.09375
- latent_norm_gain: float32 [512], replicated, may hold values from 0.1 to 1.9
- key_up_weight: bfloat16 [512, 4096], P(None, 'tp'), may hold values from -0.25 to 0.25
- value_up_weight: bfloat16 [512, 4096], P(None, 'tp'), may hold values from -0.25 to 0.25
- cached_latent_rows: bfloat16 [8, 32768, 512], P('sp', 'tp'), may hold values from -6 to 6
- past_rope: bfloat16 [8, 32768, 64], P('sp', 'tp'), may hold values from -6 to 6
- query_nope: bfloat16 [8, 4096], P('sp', 'tp'), may hold values from -8 to 8
- query_rope: bfloat16 [8, 2048], P('sp', 'tp'), may hold values from -300 to 300
Outputs:
- new_keys: bfloat16 [8, 80, 4096], P('sp', None, 'tp')
- new_values: bfloat16 [8, 80, 4096], P('sp', None, 'tp')
- new_rope: bfloat16 [8, 80, 64], P('sp')
- attended: bfloat16 [8, 4096], P('sp', 'tp')
The draws below stay inside these ranges and needn't reach their ends.
All inputs are finite; a program needn't handle non-finite values.
Results may differ from the reference program's by a relative error of at most 0.0085.
Values may be sent and summed in bfloat16 or wider, within the bound.
A program may use at most 64 MiB of HBM per device.

```python
import jax
import jax.numpy as jnp
from jax import lax

MODEL_WIDTH = 4096
HEAD_COUNT = 32
LATENT_WIDTH = 512
PLAIN_KEY_WIDTH = 128
ROPE = 64
VALUE_WIDTH = 128
PAST_POSITIONS = 32768
PROMPT_COUNT = 8
NEW = 80


def drawn_turn(key):
    turn = jnp.clip(jax.random.normal(jax.random.fold_in(key, 21), (PROMPT_COUNT, PAST_POSITIONS, ROPE), jnp.float32), -6.0, 6.0)
    return turn


def draw_past_rope(key, part):
    return drawn_turn(key).astype(jnp.bfloat16)


def draw_query_rope(key, part):
    return jnp.clip(1.5 * jax.random.normal(jax.random.fold_in(key, 25), (PROMPT_COUNT, HEAD_COUNT * ROPE), jnp.float32), -9.0, 9.0).astype(jnp.bfloat16)


def steps_of(rng, shape, shards, least, largest):
    factor_of = 1.0
    for axis_at, parts in shards:
        draws = jax.random.uniform(jax.random.fold_in(jax.random.fold_in(rng, 6), axis_at), (parts,), jnp.float32, least / len(shards), largest / len(shards))
        factor_of = factor_of * jnp.repeat(jnp.exp(draws), shape[axis_at] // parts).reshape((-1,) + (1,) * (len(shape) - 1 - axis_at))
    return factor_of


def gaussian(stream_key, extent, deviation, bound, shards=(), kind=jnp.bfloat16):
    result = deviation * jax.random.normal(stream_key, extent, jnp.float32)
    if shards:
        result = result * steps_of(stream_key, extent, shards, -0.22, 0.18)
    return jnp.clip(result, -bound, bound).astype(kind)


def setup_inputs(seed: int = 0) -> dict:
    seeds = jax.random.split(jax.random.key(seed), 11)
    tokens = gaussian(seeds[0], (PROMPT_COUNT, NEW, MODEL_WIDTH), 1.0, 6.0, ((1, 8), (2, 4)))
    latent_down_weight = gaussian(seeds[1], (MODEL_WIDTH, LATENT_WIDTH), MODEL_WIDTH ** -0.5, 0.09375)
    w_rope_key = gaussian(seeds[2], (MODEL_WIDTH, ROPE), MODEL_WIDTH ** -0.5, 0.09375)
    latent_norm_gain = jnp.clip(1.0 + 0.18 * jax.random.normal(seeds[3], (LATENT_WIDTH,), jnp.float32), 0.1, 1.9)
    key_up_weight = gaussian(seeds[4], (LATENT_WIDTH, HEAD_COUNT * PLAIN_KEY_WIDTH), LATENT_WIDTH ** -0.5, 0.25, ((1, 4),))
    value_up_weight = gaussian(seeds[5], (LATENT_WIDTH, HEAD_COUNT * VALUE_WIDTH), LATENT_WIDTH ** -0.5, 0.25, ((1, 4),))
    cached_latent_rows = gaussian(seeds[6], (PROMPT_COUNT, PAST_POSITIONS, LATENT_WIDTH), 1.0, 6.0, ((0, 8), (1, 4)))
    past_rope = draw_past_rope(jax.random.fold_in(seeds[10], 71), 0)
    query_nope = gaussian(seeds[8], (PROMPT_COUNT, HEAD_COUNT * PLAIN_KEY_WIDTH), 1.5, 8.0, ((0, 8), (1, 4)))
    query_rope = draw_query_rope(jax.random.fold_in(seeds[10], 71), 0)
    return dict(tokens=tokens, latent_down_weight=latent_down_weight, w_rope_key=w_rope_key, latent_norm_gain=latent_norm_gain, key_up_weight=key_up_weight, value_up_weight=value_up_weight, cached_latent_rows=cached_latent_rows, past_rope=past_rope, query_nope=query_nope, query_rope=query_rope)


epsilon = 1e-06
rope_theta = 10000.0

def rotate(values, positions):
    halfway = values.shape[-1] // 2
    frequency = rope_theta ** (-jnp.arange(halfway, dtype=jnp.float32) / halfway)
    angles = positions[:, None] * frequency
    first = values[..., :halfway]
    second = values[..., halfway:]
    return jnp.concatenate([first * jnp.cos(angles) - second * jnp.sin(angles), first * jnp.sin(angles) + second * jnp.cos(angles)], axis=-1)

def reference(tokens, latent_down_weight, w_rope_key, latent_norm_gain, key_up_weight, value_up_weight, cached_latent_rows, past_rope, query_nope, query_rope):
    flat = tokens.reshape(PROMPT_COUNT * NEW, MODEL_WIDTH)
    latent_raw = jnp.dot(flat, latent_down_weight, preferred_element_type=jnp.float32)
    rope_raw = jnp.dot(flat, w_rope_key, preferred_element_type=jnp.float32)
    scale = lax.rsqrt(lax.optimization_barrier(jnp.mean(latent_raw * latent_raw, axis=-1, keepdims=True)) + epsilon)
    latent = (latent_raw * scale * latent_norm_gain.astype(jnp.float32)).astype(jnp.bfloat16)
    positions = (PAST_POSITIONS + jnp.arange(NEW)).astype(jnp.float32)
    new_rope = rotate(rope_raw.reshape(PROMPT_COUNT, NEW, ROPE), positions).astype(jnp.bfloat16)
    new_keys = jnp.dot(latent, key_up_weight, preferred_element_type=jnp.float32).astype(jnp.bfloat16).reshape(PROMPT_COUNT, NEW, HEAD_COUNT * PLAIN_KEY_WIDTH)
    new_values = jnp.dot(latent, value_up_weight, preferred_element_type=jnp.float32).astype(jnp.bfloat16).reshape(PROMPT_COUNT, NEW, HEAD_COUNT * VALUE_WIDTH)
    head_keys = key_up_weight.reshape(LATENT_WIDTH, HEAD_COUNT, PLAIN_KEY_WIDTH).astype(jnp.float32)
    head_values = value_up_weight.reshape(LATENT_WIDTH, HEAD_COUNT, VALUE_WIDTH).astype(jnp.float32)
    factor = (PLAIN_KEY_WIDTH + ROPE) ** (-0.5)

    def read_sequence(items):
        query_heads, query_turn, cached, cached_turn, fresh_keys, fresh_values, fresh_turn = items
        query_heads = query_heads.astype(jnp.float32)
        query_turn = query_turn.astype(jnp.float32)
        query_latent = jnp.einsum('hd,khd->hk', query_heads, head_keys).astype(jnp.bfloat16).astype(jnp.float32)
        cached = cached.astype(jnp.float32)
        past_scores = (jnp.einsum('hk,pk->hp', query_latent, cached) + jnp.einsum('hd,pd->hp', query_turn, cached_turn.astype(jnp.float32))) * factor
        new_scores = (jnp.einsum('hd,phd->hp', query_heads, fresh_keys.astype(jnp.float32)) + jnp.einsum('hd,pd->hp', query_turn, fresh_turn.astype(jnp.float32))) * factor
        peak = jnp.maximum(lax.optimization_barrier(jnp.max(past_scores, axis=-1)), lax.optimization_barrier(jnp.max(new_scores, axis=-1)))
        past_weight = jnp.exp(past_scores - peak[:, None])
        new_weight = jnp.exp(new_scores - peak[:, None])
        denominator = lax.optimization_barrier(jnp.sum(past_weight, axis=-1)) + lax.optimization_barrier(jnp.sum(new_weight, axis=-1))
        latent_sum = jnp.einsum('hp,pk->hk', past_weight.astype(jnp.bfloat16).astype(jnp.float32), cached)
        latent_sum = latent_sum.astype(jnp.bfloat16).astype(jnp.float32)
        past_out = jnp.einsum('hk,khd->hd', latent_sum, head_values)
        new_out = jnp.einsum('hp,phd->hd', new_weight.astype(jnp.bfloat16).astype(jnp.float32), fresh_values.astype(jnp.float32))
        return ((past_out + new_out) / denominator[:, None]).astype(jnp.bfloat16).reshape(HEAD_COUNT * VALUE_WIDTH)
    attended = lax.map(read_sequence, (query_nope.reshape(PROMPT_COUNT, HEAD_COUNT, PLAIN_KEY_WIDTH), query_rope.reshape(PROMPT_COUNT, HEAD_COUNT, ROPE), cached_latent_rows, past_rope, new_keys.reshape(PROMPT_COUNT, NEW, HEAD_COUNT, PLAIN_KEY_WIDTH), new_values.reshape(PROMPT_COUNT, NEW, HEAD_COUNT, VALUE_WIDTH), new_rope))
    return (new_keys, new_values, new_rope, attended)
```

```python
import functools

import jax
import jax.numpy as jnp
import numpy as np
from jax import lax
from jax.experimental import pallas as pl
from jax.experimental.pallas import tpu as pltpu
from jax.sharding import PartitionSpec as P

PLAIN_KEY_WIDTH = 128
ROPE = 64
VALUE_WIDTH = 128
PAST_POSITIONS = 32768

epsilon = 1e-06
rope_theta = 10000.0
MESH = pl.DeviceIdType.MESH
F32 = jnp.float32
BF16 = jnp.bfloat16
LANES = 128


def up_to(n, m):
    return -(-n // m) * m


def dot(a, b, ca, cb):
    return lax.dot_general(a, b, (((ca,), (cb,)), ((), ())), preferred_element_type=F32)


def head_mask(shape, width):
    row = lax.broadcasted_iota(jnp.int32, shape, 0) * width
    col = lax.broadcasted_iota(jnp.int32, shape, 1)
    return (col >= row) & (col < row + width)


def kernel(cfg, *refs):
    (tok_h, wd_h, wr_h, gain_h, ku_h, vu_h, cache_h, prope_h, qn_h, qr_h,
     perm_h, sel_h, fold_h, table_h,
     keys_h, vals_h, rope_h, att_h,
     tok, wd, wr, gain, ku, vu, cache, prope, qn, qr, perm, sel, fold, table,
     keys_v, vals_v, rope_v, att_v,
     q_send, q_recv, part_send, part_recv, lat_send, lat_recv, a_send, a_recv, scores,
     load_sem, cache_sem, out_sem,
     q_ss, q_rs, p_ss, p_rs, l_ss, l_rs, a_ss, a_rs) = refs
    nsp, ntp, groups, npos, heads, chunk, chunks = (
        cfg[k] for k in ("nsp", "ntp", "groups", "npos", "heads", "chunk", "chunks"))
    feat, lw, gp, slot = cfg["feat"], cfg["lw"], cfg["gp"], cfg["slot"]
    s = lax.axis_index("sp")
    t = lax.axis_index("tp")
    factor = (PLAIN_KEY_WIDTH + ROPE) ** (-0.5)

    copies = {}

    def load(name, src, dst):
        c = pltpu.make_async_copy(src, dst, load_sem.at[len(copies)])
        c.start()
        copies[name] = c

    rows0 = pl.multiple_of(t * feat, LANES)
    load("qn", qn_h, qn)
    load("qr", qr_h, qr)
    load("ku", ku_h, ku)
    load("fold", fold_h, fold)
    load("tok", tok_h, tok)
    load("perm", perm_h, perm)
    load("wd", wd_h.at[pl.ds(rows0, feat), :], wd)
    load("wr", wr_h.at[:, pl.ds(rows0, feat)], wr)
    load("gain", gain_h, gain)
    load("table", table_h.at[s], table)
    load("sel", sel_h, sel)
    load("prope", prope_h, prope)
    cache_copies = []
    for c in range(chunks):
        cc = pltpu.make_async_copy(
            cache_h.at[pl.ds(c * chunk, chunk), :], cache.at[pl.ds(c * chunk, chunk), :], cache_sem.at[c])
        cc.start()
        cache_copies.append(cc)
    load("vu", vu_h, vu)

    barrier = pltpu.get_barrier_semaphore()
    for d in range(1, ntp):
        pl.semaphore_signal(barrier, inc=1, device_id=(s, lax.rem(t + d, ntp)), device_id_type=MESH)
    from_t = lax.rem(s, ntp)
    for src in range(nsp):
        @pl.when(src != s)
        def _():
            pl.semaphore_signal(barrier, inc=1, device_id=(src, from_t), device_id_type=MESH)

    for name in ("qn", "qr", "ku", "fold"):
        copies[name].wait()
    qn_row = jnp.broadcast_to(qn[...].astype(F32), (heads, qn.shape[1]))
    q_bd = jnp.where(head_mask(qn_row.shape, PLAIN_KEY_WIDTH), qn_row, 0.0).astype(BF16)
    qr_row = jnp.broadcast_to(qr[...].astype(F32), (heads, qr.shape[1]))
    qr_bd = jnp.where(head_mask(qr_row.shape, ROPE), qr_row, 0.0).astype(BF16)
    q_lat = dot(q_bd, ku[...], 1, 1).astype(BF16).astype(F32)
    q_rot = dot(qr_bd, fold[...], 1, 0)
    q_own = jnp.concatenate([q_lat, q_rot], axis=1)
    q_send[...] = q_own
    q_recv[t] = q_own

    self_row = from_t == t
    pl.semaphore_wait(
        barrier, ntp - 1 + ntp * groups - ntp * jnp.where(self_row, 1, 0).astype(jnp.int32))

    def peer_copy(src, dst, ssem, rsem, peer):
        return pltpu.make_async_remote_copy(
            src_ref=src, dst_ref=dst, send_sem=ssem, recv_sem=rsem,
            device_id=(s, peer), device_id_type=MESH)

    pending = []
    for d in range(1, ntp):
        c = peer_copy(q_send, q_recv.at[t], q_ss.at[d], q_rs.at[t], lax.rem(t + d, ntp))
        c.start()
        pending.append(c)

    for name in ("tok", "perm", "wd", "wr"):
        copies[name].wait()
    rows = dot(perm[...], tok[...], 1, 0).astype(BF16)
    lat_part = dot(rows, wd[...], 1, 0)
    rope_part = dot(rows, wr[...], 1, 1)
    for u in range(ntp):
        part_send[u, :, :lw] = lat_part[u * gp:(u + 1) * gp]
        part_send[u, :, lw:lw + ROPE] = rope_part[u * gp:(u + 1) * gp]
        part_send[u, :, lw + ROPE:] = jnp.zeros((gp, LANES - ROPE), F32)
    for d in range(1, ntp):
        peer = lax.rem(t + d, ntp)
        c = peer_copy(part_send.at[peer], part_recv.at[t], p_ss.at[d], p_rs.at[t], peer)
        c.start()
        pending.append(c)

    for d in range(1, ntp):
        peer = lax.rem(t + d, ntp)
        peer_copy(q_recv.at[peer], q_recv.at[peer], q_ss.at[d], q_rs.at[peer], peer).wait_recv()
    q_all = jnp.concatenate([q_recv[u] for u in range(ntp)], axis=0)
    q_all_lat = q_all[:, :lw].astype(BF16)
    q_all_rot = q_all[:, lw:lw + ROPE].astype(BF16)
    copies["prope"].wait()
    high = None
    for c in range(chunks):
        cache_copies[c].wait()
        cols = slice(c * chunk, (c + 1) * chunk)
        sc = (dot(q_all_lat, cache[cols, :], 1, 1) + dot(q_all_rot, prope[:, cols], 1, 0)) * factor
        scores[:, cols] = sc
        top = jnp.max(sc, axis=1, keepdims=True)
        high = top if high is None else jnp.maximum(high, top)

    total = part_send[t]
    for d in range(1, ntp):
        peer = lax.rem(t + d, ntp)
        peer_copy(part_recv.at[peer], part_recv.at[peer], p_ss.at[d], p_rs.at[peer], peer).wait_recv()
        total = total + part_recv[peer]
    copies["gain"].wait()
    copies["table"].wait()
    raw = total[:, :lw]
    scale = lax.rsqrt(jnp.mean(raw * raw, axis=-1, keepdims=True) + epsilon)
    latent = raw * scale * gain[...]
    turn = total[:, lw:lw + ROPE]
    half = ROPE // 2
    swapped = jnp.concatenate([turn[:, half:], turn[:, :half]], axis=1)
    turned = turn * table[:, :ROPE] + swapped * table[:, ROPE:]
    both = jnp.concatenate([latent, turned, jnp.zeros((gp, LANES - ROPE), F32)], axis=1)
    for k in range(groups):
        block = both[k * npos:(k + 1) * npos]
        if slot > npos:
            block = jnp.concatenate([block, jnp.zeros((slot - npos, both.shape[1]), F32)], axis=0)
        lat_send[k] = block.astype(BF16)

    def row_copy(k, d):
        return pltpu.make_async_remote_copy(
            src_ref=lat_send.at[k], dst_ref=lat_recv.at[s],
            send_sem=l_ss.at[k * ntp + d], recv_sem=l_rs.at[s],
            device_id=(k * ntp + t, lax.rem(t + d, ntp)), device_id_type=MESH)

    for k in range(groups):
        for d in range(1, ntp):
            c = row_copy(k, d)
            c.start()
            pending.append(c)

        @pl.when(k * ntp + t != s)
        def _():
            row_copy(k, 0).start()

        @pl.when(k * ntp + t == s)
        def _():
            lat_recv[s] = lat_send[k]

    summed = None
    mass = None
    for c in range(chunks):
        cols = slice(c * chunk, (c + 1) * chunk)
        w = jnp.exp(scores[:, cols] - high)
        part = jnp.sum(w, axis=1, keepdims=True)
        mass = part if mass is None else mass + part
        o = dot(w.astype(BF16), cache[cols, :], 1, 0)
        summed = o if summed is None else summed + o
    stats_lane = lax.broadcasted_iota(jnp.int32, (summed.shape[0], LANES), 1)
    stats = jnp.where(stats_lane < LANES // 2, high, mass)
    partial = jnp.concatenate([summed, stats], axis=1)
    for u in range(ntp):
        a_send[u] = partial[u * heads:(u + 1) * heads]
    for d in range(1, ntp):
        peer = lax.rem(t + d, ntp)
        c = peer_copy(a_send.at[peer], a_recv.at[t], a_ss.at[d], a_rs.at[t], peer)
        c.start()
        pending.append(c)

    for src in range(nsp):
        def arrive(src=src):
            pltpu.make_async_remote_copy(
                src_ref=lat_send.at[0], dst_ref=lat_recv.at[src],
                send_sem=l_ss.at[0], recv_sem=l_rs.at[src],
                device_id=(src, from_t), device_id_type=MESH).wait_recv()

        pl.when(jnp.logical_or(src != s, jnp.logical_not(self_row)))(arrive)
    copies["sel"].wait()
    copies["vu"].wait()
    arrived = lat_recv[...].reshape(nsp * slot, lw + LANES)
    block_lat = dot(sel[...], arrived[:, :lw], 1, 0).astype(BF16)
    new_turn = dot(arrived[:, lw:], sel[...], 0, 1)[:ROPE].astype(BF16)
    new_k = dot(block_lat, ku[...], 1, 0).astype(BF16)
    new_v = dot(block_lat, vu[...], 1, 0).astype(BF16)
    keys_v[...] = new_k
    vals_v[...] = new_v
    rope_v[...] = new_turn
    outs = [(keys_v, keys_h), (vals_v, vals_h), (rope_v, rope_h)]
    for i, (a, b) in enumerate(outs):
        pltpu.make_async_copy(a, b, out_sem.at[i]).start()

    new_scores = (dot(q_bd, new_k, 1, 1) + dot(q_rot[:, :ROPE].astype(BF16), new_turn, 1, 0)) * factor
    peak = jnp.max(new_scores, axis=1, keepdims=True)
    own = a_send[t]
    for d in range(1, ntp):
        peer = lax.rem(t + d, ntp)
        peer_copy(a_recv.at[peer], a_recv.at[peer], a_ss.at[d], a_rs.at[peer], peer).wait_recv()
    parts = [own] + [a_recv[lax.rem(t + d, ntp)] for d in range(1, ntp)]
    for p in parts:
        peak = jnp.maximum(peak, p[:, lw:lw + 1])
    new_w = jnp.exp(new_scores - peak)
    denom = jnp.sum(new_w, axis=1, keepdims=True)
    past = None
    for p in parts:
        share = jnp.exp(p[:, lw:lw + 1] - peak)
        denom = denom + p[:, lw + LANES // 2:lw + LANES // 2 + 1] * share
        o = p[:, :lw] * share
        past = o if past is None else past + o
    out = dot(past.astype(BF16), vu[...], 1, 0) + dot(new_w.astype(BF16), new_v, 1, 0)
    out = out / denom
    att_v[...] = jnp.sum(
        jnp.where(head_mask(out.shape, VALUE_WIDTH), out, 0.0), axis=0, keepdims=True).astype(BF16)
    last = pltpu.make_async_copy(att_v, att_h, out_sem.at[len(outs)])
    last.start()

    for c in pending:
        c.wait_send()
    for k in range(groups):
        @pl.when(k * ntp + t != s)
        def _():
            row_copy(k, 0).wait_send()
    for i, (a, b) in enumerate(outs):
        pltpu.make_async_copy(a, b, out_sem.at[i]).wait()
    last.wait()


def solution(mesh):
    nsp, ntp = mesh.shape["sp"], mesh.shape["tp"]

    def on_device(tokens, wd, wr, gain, ku, vu, cached, prope, qn, qr):
        prompts, npos, feat = tokens.shape
        owned, past, lw = cached.shape
        assert owned == 1 and prompts == nsp and prompts % ntp == 0
        turn = wr.shape[1]
        hk, hv = ku.shape[1], vu.shape[1]
        heads = qn.shape[1] // PLAIN_KEY_WIDTH
        groups = prompts // ntp
        gp = up_to(groups * npos, 8)
        slot = up_to(npos, 16)
        fresh = nsp * npos
        chunk = min(past, 1024)
        chunks = past // chunk
        width = lw + LANES

        perm = np.zeros((ntp * gp, prompts * npos), np.float32)
        table = np.zeros((nsp, gp, 2 * turn), np.float32)
        half = turn // 2
        freq = rope_theta ** (-np.arange(half) / half)
        for k in range(groups):
            for j in range(npos):
                i = k * npos + j
                for u in range(ntp):
                    perm[u * gp + i, j * prompts + k * ntp + u] = 1
                for sp in range(nsp):
                    a = (PAST_POSITIONS + sp * npos + j) * freq
                    table[sp, i] = np.concatenate([np.cos(a), np.cos(a), -np.sin(a), np.sin(a)])
        sel = np.zeros((fresh, nsp * slot), np.float32)
        for sp in range(nsp):
            for j in range(npos):
                sel[sp * npos + j, sp * slot + j] = 1
        fold = np.zeros((heads * turn, LANES), np.float32)
        fold[np.arange(heads * turn), np.arange(heads * turn) % turn] = 1

        cfg = dict(nsp=nsp, ntp=ntp, groups=groups, npos=npos, heads=heads, chunk=chunk,
                   chunks=chunks, feat=feat, lw=lw, gp=gp, slot=slot)
        args = (
            tokens.transpose(1, 0, 2).reshape(npos * prompts, feat),
            wd, wr.T, gain.reshape(1, lw), ku, vu,
            cached.reshape(past, lw), prope.reshape(past, turn).T, qn, qr,
            jnp.asarray(perm, BF16), jnp.asarray(sel, BF16), jnp.asarray(fold, BF16),
            jnp.asarray(table),
        )
        v = pltpu.VMEM
        dma = pltpu.SemaphoreType.DMA
        scratch = [
            v(args[0].shape, BF16), v((feat, lw), BF16), v((turn, feat), BF16), v((1, lw), F32),
            v(ku.shape, BF16), v(vu.shape, BF16), v((past, lw), BF16), v((turn, past), BF16),
            v(qn.shape, BF16), v(qr.shape, BF16),
            v(perm.shape, BF16), v(sel.shape, BF16), v(fold.shape, BF16), v(table.shape[1:], F32),
            v((fresh, hk), BF16), v((fresh, hv), BF16), v((turn, fresh), BF16), v((1, hv), BF16),
            v((heads, width), F32), v((ntp, heads, width), F32),
            v((ntp, gp, width), F32), v((ntp, gp, width), F32),
            v((groups, slot, width), BF16), v((nsp, slot, width), BF16),
            v((ntp, heads, width), F32), v((ntp, heads, width), F32),
            v((ntp * heads, past), F32),
            dma((13,)), dma((chunks,)), dma((4,)),
            dma((ntp,)), dma((ntp,)), dma((ntp,)), dma((ntp,)),
            dma((groups * ntp,)), dma((nsp,)), dma((ntp,)), dma((ntp,)),
        ]
        any_spec = pl.BlockSpec(memory_space=pl.ANY)
        keys, vals, rope, att = pl.pallas_call(
            functools.partial(kernel, cfg),
            out_shape=(
                jax.ShapeDtypeStruct((fresh, hk), BF16),
                jax.ShapeDtypeStruct((fresh, hv), BF16),
                jax.ShapeDtypeStruct((turn, fresh), BF16),
                jax.ShapeDtypeStruct((1, hv), BF16),
            ),
            in_specs=[any_spec] * len(args),
            out_specs=(any_spec,) * 4,
            scratch_shapes=scratch,
            compiler_params=pltpu.CompilerParams(
                collective_id=0, has_side_effects=True, vmem_limit_bytes=60 * 1024 * 1024),
        )(*args)
        return (
            keys.reshape(1, fresh, hk),
            vals.reshape(1, fresh, hv),
            rope.T.reshape(1, fresh, turn),
            att,
        )

    in_specs = (
        P(None, "sp", "tp"),
        P(),
        P(),
        P(),
        P(None, "tp"),
        P(None, "tp"),
        P("sp", "tp", None),
        P("sp", "tp", None),
        P("sp", "tp"),
        P("sp", "tp"),
    )
    out_specs = (P("sp", None, "tp"), P("sp", None, "tp"), P("sp", None, None), P("sp", "tp"))
    return jax.shard_map(
        on_device, mesh=mesh, in_specs=in_specs, out_specs=out_specs, check_vma=False
    )
```

```python
import functools

import jax
import jax.numpy as jnp
import numpy as np
from jax import lax
from jax.experimental import pallas as pl
from jax.experimental.pallas import tpu as pltpu
from jax.sharding import PartitionSpec as P

PLAIN_KEY_WIDTH = 128
ROPE = 64
VALUE_WIDTH = 128
PAST_POSITIONS = 32768

epsilon = 1e-06
rope_theta = 10000.0
MESH = pl.DeviceIdType.MESH
F32 = jnp.float32
BF16 = jnp.bfloat16
LANES = 128


def up_to(n, m):
    return -(-n // m) * m


def dot(a, b, ca, cb):
    return lax.dot_general(a, b, (((ca,), (cb,)), ((), ())), preferred_element_type=F32)


def head_mask(shape, width):
    row = lax.broadcasted_iota(jnp.int32, shape, 0) * width
    col = lax.broadcasted_iota(jnp.int32, shape, 1)
    return (col >= row) & (col < row + width)


def kernel(cfg, *refs):
    (tok_h, wd_h, wr_h, gain_h, ku_h, vu_h, cache_h, prope_h, qn_h, qr_h,
     perm_h, sel_h, fold_h, table_h,
     keys_v, vals_v, rope_v, att_v,
     tok, wd, wr, gain, ku, vu, cache, prope, qn, qr, perm, sel, fold, table,
     q_send, q_recv, part_send, part_recv, lat_send, lat_recv, a_send, a_recv, scores,
     load_sem, cache_sem,
     q_ss, q_rs, p_ss, p_rs, l_ss, l_rs, a_ss, a_rs) = refs
    nsp, ntp, groups, npos, heads, chunk, chunks = (
        cfg[k] for k in ("nsp", "ntp", "groups", "npos", "heads", "chunk", "chunks"))
    feat, lw, gp, slot = cfg["feat"], cfg["lw"], cfg["gp"], cfg["slot"]
    s = lax.axis_index("sp")
    t = lax.axis_index("tp")
    factor = (PLAIN_KEY_WIDTH + ROPE) ** (-0.5)

    copies = {}

    def load(name, src, dst):
        c = pltpu.make_async_copy(src, dst, load_sem.at[len(copies)])
        c.start()
        copies[name] = c

    rows0 = pl.multiple_of(t * feat, LANES)
    load("qn", qn_h, qn)
    load("qr", qr_h, qr)
    load("ku", ku_h, ku)
    load("fold", fold_h, fold)
    load("tok", tok_h, tok)
    load("perm", perm_h, perm)
    load("wd", wd_h.at[pl.ds(rows0, feat), :], wd)
    load("wr", wr_h.at[:, pl.ds(rows0, feat)], wr)
    load("gain", gain_h, gain)
    load("table", table_h.at[s], table)
    load("sel", sel_h, sel)
    load("prope", prope_h, prope)
    cache_copies = []
    for c in range(chunks):
        cc = pltpu.make_async_copy(
            cache_h.at[pl.ds(c * chunk, chunk), :], cache.at[pl.ds(c * chunk, chunk), :], cache_sem.at[c])
        cc.start()
        cache_copies.append(cc)
    load("vu", vu_h, vu)

    barrier = pltpu.get_barrier_semaphore()
    for d in range(1, ntp):
        pl.semaphore_signal(barrier, inc=1, device_id=(s, lax.rem(t + d, ntp)), device_id_type=MESH)
    from_t = lax.rem(s, ntp)
    for src in range(nsp):
        @pl.when(src != s)
        def _():
            pl.semaphore_signal(barrier, inc=1, device_id=(src, from_t), device_id_type=MESH)

    for name in ("qn", "qr", "ku", "fold"):
        copies[name].wait()
    qn_row = jnp.broadcast_to(qn[...].astype(F32), (heads, qn.shape[1]))
    q_bd = jnp.where(head_mask(qn_row.shape, PLAIN_KEY_WIDTH), qn_row, 0.0).astype(BF16)
    qr_row = jnp.broadcast_to(qr[...].astype(F32), (heads, qr.shape[1]))
    qr_bd = jnp.where(head_mask(qr_row.shape, ROPE), qr_row, 0.0).astype(BF16)
    q_lat = dot(q_bd, ku[...], 1, 1).astype(BF16).astype(F32)
    q_rot = dot(qr_bd, fold[...], 1, 0)
    q_own = jnp.concatenate([q_lat, q_rot], axis=1)
    q_send[...] = q_own
    q_recv[t] = q_own

    self_row = from_t == t
    pl.semaphore_wait(
        barrier, ntp - 1 + ntp * groups - ntp * jnp.where(self_row, 1, 0).astype(jnp.int32))

    def peer_copy(src, dst, ssem, rsem, peer):
        return pltpu.make_async_remote_copy(
            src_ref=src, dst_ref=dst, send_sem=ssem, recv_sem=rsem,
            device_id=(s, peer), device_id_type=MESH)

    pending = []
    for d in range(1, ntp):
        c = peer_copy(q_send, q_recv.at[t], q_ss.at[d], q_rs.at[t], lax.rem(t + d, ntp))
        c.start()
        pending.append(c)

    for name in ("tok", "perm", "wd", "wr"):
        copies[name].wait()
    rows = dot(perm[...], tok[...], 1, 0).astype(BF16)
    lat_part = dot(rows, wd[...], 1, 0)
    rope_part = dot(rows, wr[...], 1, 1)
    for u in range(ntp):
        part_send[u, :, :lw] = lat_part[u * gp:(u + 1) * gp]
        part_send[u, :, lw:lw + ROPE] = rope_part[u * gp:(u + 1) * gp]
        part_send[u, :, lw + ROPE:] = jnp.zeros((gp, LANES - ROPE), F32)
    for d in range(1, ntp):
        peer = lax.rem(t + d, ntp)
        c = peer_copy(part_send.at[peer], part_recv.at[t], p_ss.at[d], p_rs.at[t], peer)
        c.start()
        pending.append(c)

    for d in range(1, ntp):
        peer = lax.rem(t + d, ntp)
        peer_copy(q_recv.at[peer], q_recv.at[peer], q_ss.at[d], q_rs.at[peer], peer).wait_recv()
    q_all = jnp.concatenate([q_recv[u] for u in range(ntp)], axis=0)
    q_all_lat = q_all[:, :lw].astype(BF16)
    q_all_rot = q_all[:, lw:lw + ROPE].astype(BF16)
    copies["prope"].wait()
    high = None
    for c in range(chunks):
        cache_copies[c].wait()
        cols = slice(c * chunk, (c + 1) * chunk)
        sc = (dot(q_all_lat, cache[cols, :], 1, 1) + dot(q_all_rot, prope[:, cols], 1, 0)) * factor
        scores[:, cols] = sc
        top = jnp.max(sc, axis=1, keepdims=True)
        high = top if high is None else jnp.maximum(high, top)

    total = part_send[t]
    for d in range(1, ntp):
        peer = lax.rem(t + d, ntp)
        peer_copy(part_recv.at[peer], part_recv.at[peer], p_ss.at[d], p_rs.at[peer], peer).wait_recv()
        total = total + part_recv[peer]
    copies["gain"].wait()
    copies["table"].wait()
    raw = total[:, :lw]
    scale = lax.rsqrt(jnp.mean(raw * raw, axis=-1, keepdims=True) + epsilon)
    latent = raw * scale * gain[...]
    turn = total[:, lw:lw + ROPE]
    half = ROPE // 2
    swapped = jnp.concatenate([turn[:, half:], turn[:, :half]], axis=1)
    turned = turn * table[:, :ROPE] + swapped * table[:, ROPE:]
    both = jnp.concatenate([latent, turned, jnp.zeros((gp, LANES - ROPE), F32)], axis=1)
    for k in range(groups):
        block = both[k * npos:(k + 1) * npos]
        if slot > npos:
            block = jnp.concatenate([block, jnp.zeros((slot - npos, both.shape[1]), F32)], axis=0)
        lat_send[k] = block.astype(BF16)

    def row_copy(k, d):
        return pltpu.make_async_remote_copy(
            src_ref=lat_send.at[k], dst_ref=lat_recv.at[s],
            send_sem=l_ss.at[k * ntp + d], recv_sem=l_rs.at[s],
            device_id=(k * ntp + t, lax.rem(t + d, ntp)), device_id_type=MESH)

    for k in range(groups):
        for d in range(1, ntp):
            c = row_copy(k, d)
            c.start()
            pending.append(c)

        @pl.when(k * ntp + t != s)
        def _():
            row_copy(k, 0).start()

        @pl.when(k * ntp + t == s)
        def _():
            lat_recv[s] = lat_send[k]

    summed = None
    mass = None
    for c in range(chunks):
        cols = slice(c * chunk, (c + 1) * chunk)
        w = jnp.exp(scores[:, cols] - high)
        part = jnp.sum(w, axis=1, keepdims=True)
        mass = part if mass is None else mass + part
        o = dot(w.astype(BF16), cache[cols, :], 1, 0)
        summed = o if summed is None else summed + o
    stats_lane = lax.broadcasted_iota(jnp.int32, (summed.shape[0], LANES), 1)
    stats = jnp.where(stats_lane < LANES // 2, high, mass)
    partial = jnp.concatenate([summed, stats], axis=1)
    for u in range(ntp):
        a_send[u] = partial[u * heads:(u + 1) * heads]
    for d in range(1, ntp):
        peer = lax.rem(t + d, ntp)
        c = peer_copy(a_send.at[peer], a_recv.at[t], a_ss.at[d], a_rs.at[t], peer)
        c.start()
        pending.append(c)

    for src in range(nsp):
        def arrive(src=src):
            pltpu.make_async_remote_copy(
                src_ref=lat_send.at[0], dst_ref=lat_recv.at[src],
                send_sem=l_ss.at[0], recv_sem=l_rs.at[src],
                device_id=(src, from_t), device_id_type=MESH).wait_recv()

        pl.when(jnp.logical_or(src != s, jnp.logical_not(self_row)))(arrive)
    copies["sel"].wait()
    copies["vu"].wait()
    arrived = lat_recv[...].reshape(nsp * slot, lw + LANES)
    block_lat = dot(sel[...], arrived[:, :lw], 1, 0).astype(BF16)
    new_turn = dot(arrived[:, lw:], sel[...], 0, 1)[:ROPE].astype(BF16)
    new_k = dot(block_lat, ku[...], 1, 0).astype(BF16)
    new_v = dot(block_lat, vu[...], 1, 0).astype(BF16)
    keys_v[...] = new_k
    vals_v[...] = new_v
    rope_v[...] = new_turn

    new_scores = (dot(q_bd, new_k, 1, 1) + dot(q_rot[:, :ROPE].astype(BF16), new_turn, 1, 0)) * factor
    peak = jnp.max(new_scores, axis=1, keepdims=True)
    own = a_send[t]
    for d in range(1, ntp):
        peer = lax.rem(t + d, ntp)
        peer_copy(a_recv.at[peer], a_recv.at[peer], a_ss.at[d], a_rs.at[peer], peer).wait_recv()
    parts = [own] + [a_recv[lax.rem(t + d, ntp)] for d in range(1, ntp)]
    for p in parts:
        peak = jnp.maximum(peak, p[:, lw:lw + 1])
    new_w = jnp.exp(new_scores - peak)
    denom = jnp.sum(new_w, axis=1, keepdims=True)
    past = None
    for p in parts:
        share = jnp.exp(p[:, lw:lw + 1] - peak)
        denom = denom + p[:, lw + LANES // 2:lw + LANES // 2 + 1] * share
        o = p[:, :lw] * share
        past = o if past is None else past + o
    out = dot(past.astype(BF16), vu[...], 1, 0) + dot(new_w.astype(BF16), new_v, 1, 0)
    out = out / denom
    att_v[...] = jnp.sum(
        jnp.where(head_mask(out.shape, VALUE_WIDTH), out, 0.0), axis=0, keepdims=True).astype(BF16)

    for c in pending:
        c.wait_send()
    for k in range(groups):
        @pl.when(k * ntp + t != s)
        def _():
            row_copy(k, 0).wait_send()


def put_out(*refs):
    sem = refs[-1]
    count = (len(refs) - 1) // 2
    copies = [pltpu.make_async_copy(refs[i], refs[count + i], sem.at[i]) for i in range(count)]
    for c in copies:
        c.start()
    for c in copies:
        c.wait()


def solution(mesh):
    nsp, ntp = mesh.shape["sp"], mesh.shape["tp"]

    def on_device(tokens, wd, wr, gain, ku, vu, cached, prope, qn, qr):
        prompts, npos, feat = tokens.shape
        owned, past, lw = cached.shape
        assert owned == 1 and prompts == nsp and prompts % ntp == 0
        turn = wr.shape[1]
        hk, hv = ku.shape[1], vu.shape[1]
        heads = qn.shape[1] // PLAIN_KEY_WIDTH
        groups = prompts // ntp
        gp = up_to(groups * npos, 8)
        slot = up_to(npos, 16)
        fresh = nsp * npos
        chunk = min(past, 1024)
        chunks = past // chunk
        width = lw + LANES

        perm = np.zeros((ntp * gp, prompts * npos), np.float32)
        table = np.zeros((nsp, gp, 2 * turn), np.float32)
        half = turn // 2
        freq = rope_theta ** (-np.arange(half) / half)
        for k in range(groups):
            for j in range(npos):
                i = k * npos + j
                for u in range(ntp):
                    perm[u * gp + i, j * prompts + k * ntp + u] = 1
                for sp in range(nsp):
                    a = (PAST_POSITIONS + sp * npos + j) * freq
                    table[sp, i] = np.concatenate([np.cos(a), np.cos(a), -np.sin(a), np.sin(a)])
        sel = np.zeros((fresh, nsp * slot), np.float32)
        for sp in range(nsp):
            for j in range(npos):
                sel[sp * npos + j, sp * slot + j] = 1
        fold = np.zeros((heads * turn, LANES), np.float32)
        fold[np.arange(heads * turn), np.arange(heads * turn) % turn] = 1

        cfg = dict(nsp=nsp, ntp=ntp, groups=groups, npos=npos, heads=heads, chunk=chunk,
                   chunks=chunks, feat=feat, lw=lw, gp=gp, slot=slot)
        args = (
            tokens.transpose(1, 0, 2).reshape(npos * prompts, feat),
            wd, wr.T, gain.reshape(1, lw), ku, vu,
            cached.reshape(past, lw), prope.reshape(past, turn).T, qn, qr,
            jnp.asarray(perm, BF16), jnp.asarray(sel, BF16), jnp.asarray(fold, BF16),
            jnp.asarray(table),
        )
        v = pltpu.VMEM
        dma = pltpu.SemaphoreType.DMA
        scratch = [
            v(args[0].shape, BF16), v((feat, lw), BF16), v((turn, feat), BF16), v((1, lw), F32),
            v(ku.shape, BF16), v(vu.shape, BF16), v((past, lw), BF16), v((turn, past), BF16),
            v(qn.shape, BF16), v(qr.shape, BF16),
            v(perm.shape, BF16), v(sel.shape, BF16), v(fold.shape, BF16), v(table.shape[1:], F32),
            v((heads, width), F32), v((ntp, heads, width), F32),
            v((ntp, gp, width), F32), v((ntp, gp, width), F32),
            v((groups, slot, width), BF16), v((nsp, slot, width), BF16),
            v((ntp, heads, width), F32), v((ntp, heads, width), F32),
            v((ntp * heads, past), F32),
            dma((13,)), dma((chunks,)),
            dma((ntp,)), dma((ntp,)), dma((ntp,)), dma((ntp,)),
            dma((groups * ntp,)), dma((nsp,)), dma((ntp,)), dma((ntp,)),
        ]
        any_spec = pl.BlockSpec(memory_space=pl.ANY)
        shapes = ((fresh, hk), (fresh, hv), (turn, fresh), (1, hv))
        room = 66_900_000 - sum(2 * up_to(r, 16) * up_to(c, LANES) for r, c in shapes)
        made = pl.pallas_call(
            functools.partial(kernel, cfg),
            out_shape=tuple(pltpu.VMEM(shape, BF16) for shape in shapes),
            in_specs=[any_spec] * len(args),
            out_specs=(pl.BlockSpec(memory_space=pltpu.VMEM),) * 4,
            scratch_shapes=scratch,
            compiler_params=pltpu.CompilerParams(
                collective_id=0, has_side_effects=True, vmem_limit_bytes=room),
        )(*args)
        keys, vals, rope, att = pl.pallas_call(
            put_out,
            out_shape=tuple(jax.ShapeDtypeStruct(shape, BF16) for shape in shapes),
            in_specs=[pl.BlockSpec(memory_space=pltpu.VMEM)] * 4,
            out_specs=(any_spec,) * 4,
            scratch_shapes=[dma((4,))],
            compiler_params=pltpu.CompilerParams(vmem_limit_bytes=4 * 1024 * 1024),
        )(*made)
        return (
            keys.reshape(1, fresh, hk),
            vals.reshape(1, fresh, hv),
            rope.T.reshape(1, fresh, turn),
            att,
        )

    in_specs = (
        P(None, "sp", "tp"),
        P(),
        P(),
        P(),
        P(None, "tp"),
        P(None, "tp"),
        P("sp", "tp", None),
        P("sp", "tp", None),
        P("sp", "tp"),
        P("sp", "tp"),
    )
    out_specs = (P("sp", None, "tp"), P("sp", None, "tp"), P("sp", None, None), P("sp", "tp"))
    return jax.shard_map(
        on_device, mesh=mesh, in_specs=in_specs, out_specs=out_specs, check_vma=False
    )
```

```python
import functools

import jax
import jax.numpy as jnp
import numpy as np
from jax import lax
from jax.experimental import pallas as pl
from jax.experimental.pallas import tpu as pltpu
from jax.sharding import PartitionSpec as P

PLAIN_KEY_WIDTH = 128
ROPE = 64
VALUE_WIDTH = 128
PAST_POSITIONS = 32768

epsilon = 1e-06
rope_theta = 10000.0
MESH = pl.DeviceIdType.MESH
F32 = jnp.float32
BF16 = jnp.bfloat16
LANES = 128


def up_to(n, m):
    return -(-n // m) * m


def dot(a, b, ca, cb):
    return lax.dot_general(a, b, (((ca,), (cb,)), ((), ())), preferred_element_type=F32)


def head_mask(shape, width):
    row = lax.broadcasted_iota(jnp.int32, shape, 0) * width
    col = lax.broadcasted_iota(jnp.int32, shape, 1)
    return (col >= row) & (col < row + width)


def kernel(cfg, *refs):
    (tok_h, wd_h, wr_h, gain_h, ku_h, vu_h, cache_h, prope_h, qn_h, qr_h,
     perm_h, sel_h, fold_h, table_h,
     keys_v, vals_v, rope_v, att_v,
     tok, wd, wr, gain, ku, vu, cache, prope, qn, qr, perm, sel, fold, table,
     q_send, q_recv, part_send, part_recv, lat_send, lat_recv, a_send, a_recv, scores,
     load_sem, cache_sem,
     q_ss, q_rs, p_ss, p_rs, l_ss, l_rs, a_ss, a_rs) = refs
    nsp, ntp, groups, npos, heads, chunk, chunks = (
        cfg[k] for k in ("nsp", "ntp", "groups", "npos", "heads", "chunk", "chunks"))
    feat, lw, gp, slot = cfg["feat"], cfg["lw"], cfg["gp"], cfg["slot"]
    s = lax.axis_index("sp")
    t = lax.axis_index("tp")
    factor = (PLAIN_KEY_WIDTH + ROPE) ** (-0.5)

    copies = {}

    def load(name, src, dst):
        c = pltpu.make_async_copy(src, dst, load_sem.at[len(copies)])
        c.start()
        copies[name] = c

    rows0 = pl.multiple_of(t * feat, LANES)
    load("qn", qn_h, qn)
    load("qr", qr_h, qr)
    load("ku", ku_h, ku)
    load("fold", fold_h, fold)
    load("tok", tok_h, tok)
    load("perm", perm_h, perm)
    load("wd", wd_h.at[pl.ds(rows0, feat), :], wd)
    load("wr", wr_h.at[:, pl.ds(rows0, feat)], wr)
    load("gain", gain_h, gain)
    load("table", table_h.at[s], table)
    load("sel", sel_h, sel)
    load("prope", prope_h, prope)
    cache_copies = []
    for c in range(chunks):
        cc = pltpu.make_async_copy(
            cache_h.at[pl.ds(c * chunk, chunk), :], cache.at[pl.ds(c * chunk, chunk), :], cache_sem.at[c])
        cc.start()
        cache_copies.append(cc)
    load("vu", vu_h, vu)

    barrier = pltpu.get_barrier_semaphore()
    for d in range(1, ntp):
        pl.semaphore_signal(barrier, inc=1, device_id=(s, lax.rem(t + d, ntp)), device_id_type=MESH)
    from_t = lax.rem(s, ntp)
    for src in range(nsp):
        @pl.when(src != s)
        def _():
            pl.semaphore_signal(barrier, inc=1, device_id=(src, from_t), device_id_type=MESH)

    for name in ("qn", "qr", "ku", "fold"):
        copies[name].wait()
    qn_row = jnp.broadcast_to(qn[...].astype(F32), (heads, qn.shape[1]))
    q_bd = jnp.where(head_mask(qn_row.shape, PLAIN_KEY_WIDTH), qn_row, 0.0).astype(BF16)
    qr_row = jnp.broadcast_to(qr[...].astype(F32), (heads, qr.shape[1]))
    qr_bd = jnp.where(head_mask(qr_row.shape, ROPE), qr_row, 0.0).astype(BF16)
    q_lat = dot(q_bd, ku[...], 1, 1).astype(BF16).astype(F32)
    q_rot = dot(qr_bd, fold[...], 1, 0)
    q_own = jnp.concatenate([q_lat, q_rot], axis=1)
    q_send[...] = q_own
    q_recv[t] = q_own

    self_row = from_t == t
    pl.semaphore_wait(
        barrier, ntp - 1 + ntp * groups - ntp * jnp.where(self_row, 1, 0).astype(jnp.int32))

    def peer_copy(src, dst, ssem, rsem, peer):
        return pltpu.make_async_remote_copy(
            src_ref=src, dst_ref=dst, send_sem=ssem, recv_sem=rsem,
            device_id=(s, peer), device_id_type=MESH)

    pending = []
    for d in range(1, ntp):
        c = peer_copy(q_send, q_recv.at[t], q_ss.at[d], q_rs.at[t], lax.rem(t + d, ntp))
        c.start()
        pending.append(c)

    for name in ("tok", "perm", "wd", "wr"):
        copies[name].wait()
    rows = dot(perm[...], tok[...], 1, 0).astype(BF16)
    lat_part = dot(rows, wd[...], 1, 0)
    rope_part = dot(rows, wr[...], 1, 1)
    for u in range(ntp):
        part_send[u, :, :lw] = lat_part[u * gp:(u + 1) * gp]
        part_send[u, :, lw:lw + ROPE] = rope_part[u * gp:(u + 1) * gp]
        part_send[u, :, lw + ROPE:] = jnp.zeros((gp, LANES - ROPE), F32)
    for d in range(1, ntp):
        peer = lax.rem(t + d, ntp)
        c = peer_copy(part_send.at[peer], part_recv.at[t], p_ss.at[d], p_rs.at[t], peer)
        c.start()
        pending.append(c)

    for d in range(1, ntp):
        peer = lax.rem(t + d, ntp)
        peer_copy(q_recv.at[peer], q_recv.at[peer], q_ss.at[d], q_rs.at[peer], peer).wait_recv()
    q_all = jnp.concatenate([q_recv[u] for u in range(ntp)], axis=0)
    q_all_lat = q_all[:, :lw].astype(BF16)
    q_all_rot = q_all[:, lw:lw + ROPE].astype(BF16)
    copies["prope"].wait()
    def row_copy(k, d):
        return pltpu.make_async_remote_copy(
            src_ref=lat_send.at[k], dst_ref=lat_recv.at[s],
            send_sem=l_ss.at[k * ntp + d], recv_sem=l_rs.at[s],
            device_id=(k * ntp + t, lax.rem(t + d, ntp)), device_id_type=MESH)

    def pass_rows():
        total = part_send[t]
        for d in range(1, ntp):
            peer = lax.rem(t + d, ntp)
            peer_copy(part_recv.at[peer], part_recv.at[peer], p_ss.at[d], p_rs.at[peer], peer).wait_recv()
            total = total + part_recv[peer]
        copies["gain"].wait()
        copies["table"].wait()
        raw = total[:, :lw]
        scale = lax.rsqrt(jnp.mean(raw * raw, axis=-1, keepdims=True) + epsilon)
        latent = raw * scale * gain[...]
        turn = total[:, lw:lw + ROPE]
        half = ROPE // 2
        swapped = jnp.concatenate([turn[:, half:], turn[:, :half]], axis=1)
        turned = turn * table[:, :ROPE] + swapped * table[:, ROPE:]
        both = jnp.concatenate([latent, turned, jnp.zeros((gp, LANES - ROPE), F32)], axis=1)
        for k in range(groups):
            block = both[k * npos:(k + 1) * npos]
            if slot > npos:
                block = jnp.concatenate([block, jnp.zeros((slot - npos, both.shape[1]), F32)], axis=0)
            lat_send[k] = block.astype(BF16)

        for k in range(groups):
            for d in range(1, ntp):
                c = row_copy(k, d)
                c.start()
                pending.append(c)

            @pl.when(k * ntp + t != s)
            def _():
                row_copy(k, 0).start()

            @pl.when(k * ntp + t == s)
            def _():
                lat_recv[s] = lat_send[k]

    high = None
    for c in range(chunks):
        if c == chunks // 2:
            pass_rows()
        cache_copies[c].wait()
        cols = slice(c * chunk, (c + 1) * chunk)
        sc = (dot(q_all_lat, cache[cols, :], 1, 1) + dot(q_all_rot, prope[:, cols], 1, 0)) * factor
        scores[:, cols] = sc
        top = jnp.max(sc, axis=1, keepdims=True)
        high = top if high is None else jnp.maximum(high, top)

    summed = None
    mass = None
    for c in range(chunks):
        cols = slice(c * chunk, (c + 1) * chunk)
        w = jnp.exp(scores[:, cols] - high)
        part = jnp.sum(w, axis=1, keepdims=True)
        mass = part if mass is None else mass + part
        o = dot(w.astype(BF16), cache[cols, :], 1, 0)
        summed = o if summed is None else summed + o
    stats_lane = lax.broadcasted_iota(jnp.int32, (summed.shape[0], LANES), 1)
    stats = jnp.where(stats_lane < LANES // 2, high, mass)
    partial = jnp.concatenate([summed, stats], axis=1)
    for u in range(ntp):
        a_send[u] = partial[u * heads:(u + 1) * heads]
    for d in range(1, ntp):
        peer = lax.rem(t + d, ntp)
        c = peer_copy(a_send.at[peer], a_recv.at[t], a_ss.at[d], a_rs.at[t], peer)
        c.start()
        pending.append(c)

    for src in range(nsp):
        def arrive(src=src):
            pltpu.make_async_remote_copy(
                src_ref=lat_send.at[0], dst_ref=lat_recv.at[src],
                send_sem=l_ss.at[0], recv_sem=l_rs.at[src],
                device_id=(src, from_t), device_id_type=MESH).wait_recv()

        pl.when(jnp.logical_or(src != s, jnp.logical_not(self_row)))(arrive)
    copies["sel"].wait()
    copies["vu"].wait()
    arrived = lat_recv[...].reshape(nsp * slot, lw + LANES)
    block_lat = dot(sel[...], arrived[:, :lw], 1, 0).astype(BF16)
    new_turn = dot(arrived[:, lw:], sel[...], 0, 1)[:ROPE].astype(BF16)
    new_k = dot(block_lat, ku[...], 1, 0).astype(BF16)
    new_v = dot(block_lat, vu[...], 1, 0).astype(BF16)
    keys_v[...] = new_k
    vals_v[...] = new_v
    rope_v[...] = new_turn

    new_scores = (dot(q_bd, new_k, 1, 1) + dot(q_rot[:, :ROPE].astype(BF16), new_turn, 1, 0)) * factor
    peak = jnp.max(new_scores, axis=1, keepdims=True)
    own = a_send[t]
    for d in range(1, ntp):
        peer = lax.rem(t + d, ntp)
        peer_copy(a_recv.at[peer], a_recv.at[peer], a_ss.at[d], a_rs.at[peer], peer).wait_recv()
    parts = [own] + [a_recv[lax.rem(t + d, ntp)] for d in range(1, ntp)]
    for p in parts:
        peak = jnp.maximum(peak, p[:, lw:lw + 1])
    new_w = jnp.exp(new_scores - peak)
    denom = jnp.sum(new_w, axis=1, keepdims=True)
    past = None
    for p in parts:
        share = jnp.exp(p[:, lw:lw + 1] - peak)
        denom = denom + p[:, lw + LANES // 2:lw + LANES // 2 + 1] * share
        o = p[:, :lw] * share
        past = o if past is None else past + o
    out = dot(past.astype(BF16), vu[...], 1, 0) + dot(new_w.astype(BF16), new_v, 1, 0)
    out = out / denom
    att_v[...] = jnp.sum(
        jnp.where(head_mask(out.shape, VALUE_WIDTH), out, 0.0), axis=0, keepdims=True).astype(BF16)

    for c in pending:
        c.wait_send()
    for k in range(groups):
        @pl.when(k * ntp + t != s)
        def _():
            row_copy(k, 0).wait_send()


def put_out(*refs):
    sem = refs[-1]
    count = (len(refs) - 1) // 2
    copies = [pltpu.make_async_copy(refs[i], refs[count + i], sem.at[i]) for i in range(count)]
    for c in copies:
        c.start()
    for c in copies:
        c.wait()


def solution(mesh):
    nsp, ntp = mesh.shape["sp"], mesh.shape["tp"]

    def on_device(tokens, wd, wr, gain, ku, vu, cached, prope, qn, qr):
        prompts, npos, feat = tokens.shape
        owned, past, lw = cached.shape
        assert owned == 1 and prompts == nsp and prompts % ntp == 0
        turn = wr.shape[1]
        hk, hv = ku.shape[1], vu.shape[1]
        heads = qn.shape[1] // PLAIN_KEY_WIDTH
        groups = prompts // ntp
        gp = up_to(groups * npos, 8)
        slot = up_to(npos, 16)
        fresh = nsp * npos
        chunk = min(past, 1024)
        chunks = past // chunk
        width = lw + LANES

        perm = np.zeros((ntp * gp, prompts * npos), np.float32)
        table = np.zeros((nsp, gp, 2 * turn), np.float32)
        half = turn // 2
        freq = rope_theta ** (-np.arange(half) / half)
        for k in range(groups):
            for j in range(npos):
                i = k * npos + j
                for u in range(ntp):
                    perm[u * gp + i, j * prompts + k * ntp + u] = 1
                for sp in range(nsp):
                    a = (PAST_POSITIONS + sp * npos + j) * freq
                    table[sp, i] = np.concatenate([np.cos(a), np.cos(a), -np.sin(a), np.sin(a)])
        sel = np.zeros((fresh, nsp * slot), np.float32)
        for sp in range(nsp):
            for j in range(npos):
                sel[sp * npos + j, sp * slot + j] = 1
        fold = np.zeros((heads * turn, LANES), np.float32)
        fold[np.arange(heads * turn), np.arange(heads * turn) % turn] = 1

        cfg = dict(nsp=nsp, ntp=ntp, groups=groups, npos=npos, heads=heads, chunk=chunk,
                   chunks=chunks, feat=feat, lw=lw, gp=gp, slot=slot)
        args = (
            tokens.transpose(1, 0, 2).reshape(npos * prompts, feat),
            wd, wr.T, gain.reshape(1, lw), ku, vu,
            cached.reshape(past, lw), prope.reshape(past, turn).T, qn, qr,
            jnp.asarray(perm, BF16), jnp.asarray(sel, BF16), jnp.asarray(fold, BF16),
            jnp.asarray(table),
        )
        v = pltpu.VMEM
        dma = pltpu.SemaphoreType.DMA
        scratch = [
            v(args[0].shape, BF16), v((feat, lw), BF16), v((turn, feat), BF16), v((1, lw), F32),
            v(ku.shape, BF16), v(vu.shape, BF16), v((past, lw), BF16), v((turn, past), BF16),
            v(qn.shape, BF16), v(qr.shape, BF16),
            v(perm.shape, BF16), v(sel.shape, BF16), v(fold.shape, BF16), v(table.shape[1:], F32),
            v((heads, width), F32), v((ntp, heads, width), F32),
            v((ntp, gp, width), F32), v((ntp, gp, width), F32),
            v((groups, slot, width), BF16), v((nsp, slot, width), BF16),
            v((ntp, heads, width), F32), v((ntp, heads, width), F32),
            v((ntp * heads, past), F32),
            dma((13,)), dma((chunks,)),
            dma((ntp,)), dma((ntp,)), dma((ntp,)), dma((ntp,)),
            dma((groups * ntp,)), dma((nsp,)), dma((ntp,)), dma((ntp,)),
        ]
        any_spec = pl.BlockSpec(memory_space=pl.ANY)
        shapes = ((fresh, hk), (fresh, hv), (turn, fresh), (1, hv))
        room = 66_900_000 - sum(2 * up_to(r, 16) * up_to(c, LANES) for r, c in shapes)
        made = pl.pallas_call(
            functools.partial(kernel, cfg),
            out_shape=tuple(pltpu.VMEM(shape, BF16) for shape in shapes),
            in_specs=[any_spec] * len(args),
            out_specs=(pl.BlockSpec(memory_space=pltpu.VMEM),) * 4,
            scratch_shapes=scratch,
            compiler_params=pltpu.CompilerParams(
                collective_id=0, has_side_effects=True, vmem_limit_bytes=room),
        )(*args)
        keys, vals, rope, att = pl.pallas_call(
            put_out,
            out_shape=tuple(jax.ShapeDtypeStruct(shape, BF16) for shape in shapes),
            in_specs=[pl.BlockSpec(memory_space=pltpu.VMEM)] * 4,
            out_specs=(any_spec,) * 4,
            scratch_shapes=[dma((4,))],
            compiler_params=pltpu.CompilerParams(vmem_limit_bytes=4 * 1024 * 1024),
        )(*made)
        return (
            keys.reshape(1, fresh, hk),
            vals.reshape(1, fresh, hv),
            rope.T.reshape(1, fresh, turn),
            att,
        )

    in_specs = (
        P(None, "sp", "tp"),
        P(),
        P(),
        P(),
        P(None, "tp"),
        P(None, "tp"),
        P("sp", "tp", None),
        P("sp", "tp", None),
        P("sp", "tp"),
        P("sp", "tp"),
    )
    out_specs = (P("sp", None, "tp"), P("sp", None, "tp"), P("sp", None, None), P("sp", "tp"))
    return jax.shard_map(
        on_device, mesh=mesh, in_specs=in_specs, out_specs=out_specs, check_vma=False
    )
```

```python
import functools

import jax
import jax.numpy as jnp
import numpy as np
from jax import lax
from jax.experimental import pallas as pl
from jax.experimental.pallas import tpu as pltpu
from jax.sharding import PartitionSpec as P

PLAIN_KEY_WIDTH = 128
ROPE = 64
VALUE_WIDTH = 128
PAST_POSITIONS = 32768

epsilon = 1e-06
rope_theta = 10000.0
MESH = pl.DeviceIdType.MESH
F32 = jnp.float32
BF16 = jnp.bfloat16
LANES = 128


def up_to(n, m):
    return -(-n // m) * m


def dot(a, b, ca, cb):
    return lax.dot_general(a, b, (((ca,), (cb,)), ((), ())), preferred_element_type=F32)


def head_mask(shape, width):
    row = lax.broadcasted_iota(jnp.int32, shape, 0) * width
    col = lax.broadcasted_iota(jnp.int32, shape, 1)
    return (col >= row) & (col < row + width)


def kernel(cfg, *refs):
    (tok_h, wd_h, wr_h, gain_h, ku_h, vu_h, cache_h, prope_h, qn_h, qr_h,
     perm_h, sel_h, fold_h, table_h,
     keys_v, vals_v, rope_v, att_v,
     tok, wd, wr, gain, ku, vu, cache, prope, qn, qr, perm, sel, fold, table,
     q_send, q_recv, part_send, part_recv, lat_send, lat_recv, a_send, a_recv, scores,
     load_sem, cache_sem,
     q_ss, q_rs, p_ss, p_rs, l_ss, l_rs, a_ss, a_rs) = refs
    nsp, ntp, groups, npos, heads, chunk, chunks = (
        cfg[k] for k in ("nsp", "ntp", "groups", "npos", "heads", "chunk", "chunks"))
    feat, lw, gp, slot = cfg["feat"], cfg["lw"], cfg["gp"], cfg["slot"]
    s = lax.axis_index("sp")
    t = lax.axis_index("tp")
    factor = (PLAIN_KEY_WIDTH + ROPE) ** (-0.5)

    copies = {}

    def load(name, src, dst):
        c = pltpu.make_async_copy(src, dst, load_sem.at[len(copies)])
        c.start()
        copies[name] = c

    rows0 = pl.multiple_of(t * feat, LANES)
    load("qn", qn_h, qn)
    load("qr", qr_h, qr)
    load("ku", ku_h, ku)
    load("fold", fold_h, fold)
    load("tok", tok_h, tok)
    load("perm", perm_h, perm)
    load("wd", wd_h.at[pl.ds(rows0, feat), :], wd)
    load("wr", wr_h.at[:, pl.ds(rows0, feat)], wr)
    load("gain", gain_h, gain)
    load("table", table_h.at[s], table)
    load("sel", sel_h, sel)
    load("prope", prope_h, prope)
    cache_copies = []
    for c in range(chunks):
        cc = pltpu.make_async_copy(
            cache_h.at[pl.ds(c * chunk, chunk), :], cache.at[pl.ds(c * chunk, chunk), :], cache_sem.at[c])
        cc.start()
        cache_copies.append(cc)
    load("vu", vu_h, vu)

    barrier = pltpu.get_barrier_semaphore()
    for d in range(1, ntp):
        pl.semaphore_signal(barrier, inc=1, device_id=(s, lax.rem(t + d, ntp)), device_id_type=MESH)
    from_t = lax.rem(s, ntp)
    for src in range(nsp):
        @pl.when(src != s)
        def _():
            pl.semaphore_signal(barrier, inc=1, device_id=(src, from_t), device_id_type=MESH)

    for name in ("qn", "qr", "ku", "fold"):
        copies[name].wait()
    qn_row = jnp.broadcast_to(qn[...].astype(F32), (heads, qn.shape[1]))
    q_bd = jnp.where(head_mask(qn_row.shape, PLAIN_KEY_WIDTH), qn_row, 0.0).astype(BF16)
    qr_row = jnp.broadcast_to(qr[...].astype(F32), (heads, qr.shape[1]))
    qr_bd = jnp.where(head_mask(qr_row.shape, ROPE), qr_row, 0.0).astype(BF16)
    q_lat = dot(q_bd, ku[...], 1, 1).astype(BF16).astype(F32)
    q_rot = dot(qr_bd, fold[...], 1, 0)
    q_own = jnp.concatenate([q_lat, q_rot], axis=1)
    q_send[...] = q_own
    q_recv[t] = q_own

    self_row = from_t == t
    pl.semaphore_wait(
        barrier, ntp - 1 + ntp * groups - ntp * jnp.where(self_row, 1, 0).astype(jnp.int32))

    def peer_copy(src, dst, ssem, rsem, peer):
        return pltpu.make_async_remote_copy(
            src_ref=src, dst_ref=dst, send_sem=ssem, recv_sem=rsem,
            device_id=(s, peer), device_id_type=MESH)

    pending = []
    for d in range(1, ntp):
        c = peer_copy(q_send, q_recv.at[t], q_ss.at[d], q_rs.at[t], lax.rem(t + d, ntp))
        c.start()
        pending.append(c)

    for name in ("tok", "perm", "wd", "wr"):
        copies[name].wait()
    rows = dot(perm[...], tok[...], 1, 0).astype(BF16)
    lat_part = dot(rows, wd[...], 1, 0)
    rope_part = dot(rows, wr[...], 1, 1)
    for u in range(ntp):
        part_send[u, :, :lw] = lat_part[u * gp:(u + 1) * gp]
        part_send[u, :, lw:lw + ROPE] = rope_part[u * gp:(u + 1) * gp]
        part_send[u, :, lw + ROPE:] = jnp.zeros((gp, LANES - ROPE), F32)
    for d in range(1, ntp):
        peer = lax.rem(t + d, ntp)
        c = peer_copy(part_send.at[peer], part_recv.at[t], p_ss.at[d], p_rs.at[t], peer)
        c.start()
        pending.append(c)

    for d in range(1, ntp):
        peer = lax.rem(t + d, ntp)
        peer_copy(q_recv.at[peer], q_recv.at[peer], q_ss.at[d], q_rs.at[peer], peer).wait_recv()
    q_all = jnp.concatenate([q_recv[u] for u in range(ntp)], axis=0)
    q_all_lat = q_all[:, :lw].astype(BF16)
    q_all_rot = q_all[:, lw:lw + ROPE].astype(BF16)
    copies["prope"].wait()
    def row_copy(k, d):
        return pltpu.make_async_remote_copy(
            src_ref=lat_send.at[k], dst_ref=lat_recv.at[s],
            send_sem=l_ss.at[k * ntp + d], recv_sem=l_rs.at[s],
            device_id=(k * ntp + t, lax.rem(t + d, ntp)), device_id_type=MESH)

    def pass_rows():
        total = part_send[t]
        for d in range(1, ntp):
            peer = lax.rem(t + d, ntp)
            peer_copy(part_recv.at[peer], part_recv.at[peer], p_ss.at[d], p_rs.at[peer], peer).wait_recv()
            total = total + part_recv[peer]
        copies["gain"].wait()
        copies["table"].wait()
        raw = total[:, :lw]
        scale = lax.rsqrt(jnp.mean(raw * raw, axis=-1, keepdims=True) + epsilon)
        latent = raw * scale * gain[...]
        turn = total[:, lw:lw + ROPE]
        half = ROPE // 2
        swapped = jnp.concatenate([turn[:, half:], turn[:, :half]], axis=1)
        turned = turn * table[:, :ROPE] + swapped * table[:, ROPE:]
        both = jnp.concatenate([latent, turned, jnp.zeros((gp, LANES - ROPE), F32)], axis=1)
        for k in range(groups):
            block = both[k * npos:(k + 1) * npos]
            if slot > npos:
                block = jnp.concatenate([block, jnp.zeros((slot - npos, both.shape[1]), F32)], axis=0)
            lat_send[k] = block.astype(BF16)

        for k in range(groups):
            for d in range(1, ntp):
                c = row_copy(k, d)
                c.start()
                pending.append(c)

            @pl.when(k * ntp + t != s)
            def _():
                row_copy(k, 0).start()

            @pl.when(k * ntp + t == s)
            def _():
                lat_recv[s] = lat_send[k]

    high = None
    for c in range(chunks):
        if c == chunks // 4:
            pass_rows()
        cache_copies[c].wait()
        cols = slice(c * chunk, (c + 1) * chunk)
        sc = (dot(q_all_lat, cache[cols, :], 1, 1) + dot(q_all_rot, prope[:, cols], 1, 0)) * factor
        scores[:, cols] = sc
        top = jnp.max(sc, axis=1, keepdims=True)
        high = top if high is None else jnp.maximum(high, top)

    summed = None
    mass = None
    for c in range(chunks):
        cols = slice(c * chunk, (c + 1) * chunk)
        w = jnp.exp(scores[:, cols] - high)
        part = jnp.sum(w, axis=1, keepdims=True)
        mass = part if mass is None else mass + part
        o = dot(w.astype(BF16), cache[cols, :], 1, 0)
        summed = o if summed is None else summed + o
    stats_lane = lax.broadcasted_iota(jnp.int32, (summed.shape[0], LANES), 1)
    stats = jnp.where(stats_lane < LANES // 2, high, mass)
    partial = jnp.concatenate([summed, stats], axis=1)
    for u in range(ntp):
        a_send[u] = partial[u * heads:(u + 1) * heads]
    for d in range(1, ntp):
        peer = lax.rem(t + d, ntp)
        c = peer_copy(a_send.at[peer], a_recv.at[t], a_ss.at[d], a_rs.at[t], peer)
        c.start()
        pending.append(c)

    for src in range(nsp):
        def arrive(src=src):
            pltpu.make_async_remote_copy(
                src_ref=lat_send.at[0], dst_ref=lat_recv.at[src],
                send_sem=l_ss.at[0], recv_sem=l_rs.at[src],
                device_id=(src, from_t), device_id_type=MESH).wait_recv()

        pl.when(jnp.logical_or(src != s, jnp.logical_not(self_row)))(arrive)
    copies["sel"].wait()
    copies["vu"].wait()
    arrived = lat_recv[...].reshape(nsp * slot, lw + LANES)
    block_lat = dot(sel[...], arrived[:, :lw], 1, 0).astype(BF16)
    new_turn = dot(arrived[:, lw:], sel[...], 0, 1)[:ROPE].astype(BF16)
    new_k = dot(block_lat, ku[...], 1, 0).astype(BF16)
    new_v = dot(block_lat, vu[...], 1, 0).astype(BF16)
    keys_v[...] = new_k
    vals_v[...] = new_v
    rope_v[...] = new_turn

    new_scores = (dot(q_bd, new_k, 1, 1) + dot(q_rot[:, :ROPE].astype(BF16), new_turn, 1, 0)) * factor
    peak = jnp.max(new_scores, axis=1, keepdims=True)
    own = a_send[t]
    for d in range(1, ntp):
        peer = lax.rem(t + d, ntp)
        peer_copy(a_recv.at[peer], a_recv.at[peer], a_ss.at[d], a_rs.at[peer], peer).wait_recv()
    parts = [own] + [a_recv[lax.rem(t + d, ntp)] for d in range(1, ntp)]
    for p in parts:
        peak = jnp.maximum(peak, p[:, lw:lw + 1])
    new_w = jnp.exp(new_scores - peak)
    denom = jnp.sum(new_w, axis=1, keepdims=True)
    past = None
    for p in parts:
        share = jnp.exp(p[:, lw:lw + 1] - peak)
        denom = denom + p[:, lw + LANES // 2:lw + LANES // 2 + 1] * share
        o = p[:, :lw] * share
        past = o if past is None else past + o
    out = dot(past.astype(BF16), vu[...], 1, 0) + dot(new_w.astype(BF16), new_v, 1, 0)
    out = out / denom
    att_v[...] = jnp.sum(
        jnp.where(head_mask(out.shape, VALUE_WIDTH), out, 0.0), axis=0, keepdims=True).astype(BF16)

    for c in pending:
        c.wait_send()
    for k in range(groups):
        @pl.when(k * ntp + t != s)
        def _():
            row_copy(k, 0).wait_send()


def put_out(*refs):
    sem = refs[-1]
    count = (len(refs) - 1) // 2
    copies = [pltpu.make_async_copy(refs[i], refs[count + i], sem.at[i]) for i in range(count)]
    for c in copies:
        c.start()
    for c in copies:
        c.wait()


def solution(mesh):
    nsp, ntp = mesh.shape["sp"], mesh.shape["tp"]

    def on_device(tokens, wd, wr, gain, ku, vu, cached, prope, qn, qr):
        prompts, npos, feat = tokens.shape
        owned, past, lw = cached.shape
        assert owned == 1 and prompts == nsp and prompts % ntp == 0
        turn = wr.shape[1]
        hk, hv = ku.shape[1], vu.shape[1]
        heads = qn.shape[1] // PLAIN_KEY_WIDTH
        groups = prompts // ntp
        gp = up_to(groups * npos, 8)
        slot = up_to(npos, 16)
        fresh = nsp * npos
        chunk = min(past, 1024)
        chunks = past // chunk
        width = lw + LANES

        perm = np.zeros((ntp * gp, prompts * npos), np.float32)
        table = np.zeros((nsp, gp, 2 * turn), np.float32)
        half = turn // 2
        freq = rope_theta ** (-np.arange(half) / half)
        for k in range(groups):
            for j in range(npos):
                i = k * npos + j
                for u in range(ntp):
                    perm[u * gp + i, j * prompts + k * ntp + u] = 1
                for sp in range(nsp):
                    a = (PAST_POSITIONS + sp * npos + j) * freq
                    table[sp, i] = np.concatenate([np.cos(a), np.cos(a), -np.sin(a), np.sin(a)])
        sel = np.zeros((fresh, nsp * slot), np.float32)
        for sp in range(nsp):
            for j in range(npos):
                sel[sp * npos + j, sp * slot + j] = 1
        fold = np.zeros((heads * turn, LANES), np.float32)
        fold[np.arange(heads * turn), np.arange(heads * turn) % turn] = 1

        cfg = dict(nsp=nsp, ntp=ntp, groups=groups, npos=npos, heads=heads, chunk=chunk,
                   chunks=chunks, feat=feat, lw=lw, gp=gp, slot=slot)
        args = (
            tokens.transpose(1, 0, 2).reshape(npos * prompts, feat),
            wd, wr.T, gain.reshape(1, lw), ku, vu,
            cached.reshape(past, lw), prope.reshape(past, turn).T, qn, qr,
            jnp.asarray(perm, BF16), jnp.asarray(sel, BF16), jnp.asarray(fold, BF16),
            jnp.asarray(table),
        )
        v = pltpu.VMEM
        dma = pltpu.SemaphoreType.DMA
        scratch = [
            v(args[0].shape, BF16), v((feat, lw), BF16), v((turn, feat), BF16), v((1, lw), F32),
            v(ku.shape, BF16), v(vu.shape, BF16), v((past, lw), BF16), v((turn, past), BF16),
            v(qn.shape, BF16), v(qr.shape, BF16),
            v(perm.shape, BF16), v(sel.shape, BF16), v(fold.shape, BF16), v(table.shape[1:], F32),
            v((heads, width), F32), v((ntp, heads, width), F32),
            v((ntp, gp, width), F32), v((ntp, gp, width), F32),
            v((groups, slot, width), BF16), v((nsp, slot, width), BF16),
            v((ntp, heads, width), F32), v((ntp, heads, width), F32),
            v((ntp * heads, past), F32),
            dma((13,)), dma((chunks,)),
            dma((ntp,)), dma((ntp,)), dma((ntp,)), dma((ntp,)),
            dma((groups * ntp,)), dma((nsp,)), dma((ntp,)), dma((ntp,)),
        ]
        any_spec = pl.BlockSpec(memory_space=pl.ANY)
        shapes = ((fresh, hk), (fresh, hv), (turn, fresh), (1, hv))
        room = 66_900_000 - sum(2 * up_to(r, 16) * up_to(c, LANES) for r, c in shapes)
        made = pl.pallas_call(
            functools.partial(kernel, cfg),
            out_shape=tuple(pltpu.VMEM(shape, BF16) for shape in shapes),
            in_specs=[any_spec] * len(args),
            out_specs=(pl.BlockSpec(memory_space=pltpu.VMEM),) * 4,
            scratch_shapes=scratch,
            compiler_params=pltpu.CompilerParams(
                collective_id=0, has_side_effects=True, vmem_limit_bytes=room),
        )(*args)
        keys, vals, rope, att = pl.pallas_call(
            put_out,
            out_shape=tuple(jax.ShapeDtypeStruct(shape, BF16) for shape in shapes),
            in_specs=[pl.BlockSpec(memory_space=pltpu.VMEM)] * 4,
            out_specs=(any_spec,) * 4,
            scratch_shapes=[dma((4,))],
            compiler_params=pltpu.CompilerParams(vmem_limit_bytes=4 * 1024 * 1024),
        )(*made)
        return (
            keys.reshape(1, fresh, hk),
            vals.reshape(1, fresh, hv),
            rope.T.reshape(1, fresh, turn),
            att,
        )

    in_specs = (
        P(None, "sp", "tp"),
        P(),
        P(),
        P(),
        P(None, "tp"),
        P(None, "tp"),
        P("sp", "tp", None),
        P("sp", "tp", None),
        P("sp", "tp"),
        P("sp", "tp"),
    )
    out_specs = (P("sp", None, "tp"), P("sp", None, "tp"), P("sp", None, None), P("sp", "tp"))
    return jax.shard_map(
        on_device, mesh=mesh, in_specs=in_specs, out_specs=out_specs, check_vma=False
    )
```

```python
import functools

import jax
import jax.numpy as jnp
import numpy as np
from jax import lax
from jax.experimental import pallas as pl
from jax.experimental.pallas import tpu as pltpu
from jax.sharding import PartitionSpec as P

PLAIN_KEY_WIDTH = 128
ROPE = 64
VALUE_WIDTH = 128
PAST_POSITIONS = 32768

epsilon = 1e-06
rope_theta = 10000.0
MESH = pl.DeviceIdType.MESH
F32 = jnp.float32
BF16 = jnp.bfloat16
LANES = 128


def up_to(n, m):
    return -(-n // m) * m


def dot(a, b, ca, cb):
    return lax.dot_general(a, b, (((ca,), (cb,)), ((), ())), preferred_element_type=F32)


def head_mask(shape, width):
    row = lax.broadcasted_iota(jnp.int32, shape, 0) * width
    col = lax.broadcasted_iota(jnp.int32, shape, 1)
    return (col >= row) & (col < row + width)


def kernel(cfg, *refs):
    (tok_h, wd_h, wr_h, gain_h, ku_h, vu_h, cache_h, prope_h, qn_h, qr_h,
     perm_h, sel_h, fold_h, table_h,
     keys_v, vals_v, rope_v, att_v,
     tok, wd, wr, gain, ku, vu, cache, prope, qn, qr, perm, sel, fold, table,
     q_send, q_recv, part_send, part_recv, lat_send, lat_recv, a_send, a_recv, scores,
     load_sem, cache_sem,
     q_ss, q_rs, p_ss, p_rs, l_ss, l_rs, a_ss, a_rs) = refs
    nsp, ntp, groups, npos, heads, chunk, chunks = (
        cfg[k] for k in ("nsp", "ntp", "groups", "npos", "heads", "chunk", "chunks"))
    feat, lw, gp, slot = cfg["feat"], cfg["lw"], cfg["gp"], cfg["slot"]
    s = lax.axis_index("sp")
    t = lax.axis_index("tp")
    factor = (PLAIN_KEY_WIDTH + ROPE) ** (-0.5)

    copies = {}

    def load(name, src, dst):
        c = pltpu.make_async_copy(src, dst, load_sem.at[len(copies)])
        c.start()
        copies[name] = c

    rows0 = pl.multiple_of(t * feat, LANES)
    load("qn", qn_h, qn)
    load("qr", qr_h, qr)
    load("ku", ku_h, ku)
    load("fold", fold_h, fold)
    load("tok", tok_h, tok)
    load("perm", perm_h, perm)
    load("wd", wd_h.at[pl.ds(rows0, feat), :], wd)
    load("wr", wr_h.at[:, pl.ds(rows0, feat)], wr)
    load("gain", gain_h, gain)
    load("table", table_h.at[s], table)
    load("sel", sel_h, sel)
    load("prope", prope_h, prope)
    cache_copies = []
    for c in range(chunks):
        cc = pltpu.make_async_copy(
            cache_h.at[pl.ds(c * chunk, chunk), :], cache.at[pl.ds(c * chunk, chunk), :], cache_sem.at[c])
        cc.start()
        cache_copies.append(cc)
    load("vu", vu_h, vu)

    barrier = pltpu.get_barrier_semaphore()
    for d in range(1, ntp):
        pl.semaphore_signal(barrier, inc=1, device_id=(s, lax.rem(t + d, ntp)), device_id_type=MESH)
    from_t = lax.rem(s, ntp)
    for src in range(nsp):
        @pl.when(src != s)
        def _():
            pl.semaphore_signal(barrier, inc=1, device_id=(src, from_t), device_id_type=MESH)

    for name in ("qn", "qr", "ku", "fold"):
        copies[name].wait()
    qn_row = jnp.broadcast_to(qn[...].astype(F32), (heads, qn.shape[1]))
    q_bd = jnp.where(head_mask(qn_row.shape, PLAIN_KEY_WIDTH), qn_row, 0.0).astype(BF16)
    qr_row = jnp.broadcast_to(qr[...].astype(F32), (heads, qr.shape[1]))
    qr_bd = jnp.where(head_mask(qr_row.shape, ROPE), qr_row, 0.0).astype(BF16)
    q_lat = dot(q_bd, ku[...], 1, 1).astype(BF16).astype(F32)
    q_rot = dot(qr_bd, fold[...], 1, 0)
    q_own = jnp.concatenate([q_lat, q_rot], axis=1)
    q_send[...] = q_own
    q_recv[t] = q_own

    for name in ("tok", "perm", "wd", "wr"):
        copies[name].wait()
    rows = dot(perm[...], tok[...], 1, 0).astype(BF16)
    lat_part = dot(rows, wd[...], 1, 0)
    rope_part = dot(rows, wr[...], 1, 1)
    for u in range(ntp):
        part_send[u, :, :lw] = lat_part[u * gp:(u + 1) * gp]
        part_send[u, :, lw:lw + ROPE] = rope_part[u * gp:(u + 1) * gp]
        part_send[u, :, lw + ROPE:] = jnp.zeros((gp, LANES - ROPE), F32)
    self_row = from_t == t
    pl.semaphore_wait(
        barrier, ntp - 1 + ntp * groups - ntp * jnp.where(self_row, 1, 0).astype(jnp.int32))

    def peer_copy(src, dst, ssem, rsem, peer):
        return pltpu.make_async_remote_copy(
            src_ref=src, dst_ref=dst, send_sem=ssem, recv_sem=rsem,
            device_id=(s, peer), device_id_type=MESH)

    pending = []
    for d in range(1, ntp):
        c = peer_copy(q_send, q_recv.at[t], q_ss.at[d], q_rs.at[t], lax.rem(t + d, ntp))
        c.start()
        pending.append(c)
    for d in range(1, ntp):
        peer = lax.rem(t + d, ntp)
        c = peer_copy(part_send.at[peer], part_recv.at[t], p_ss.at[d], p_rs.at[t], peer)
        c.start()
        pending.append(c)

    for d in range(1, ntp):
        peer = lax.rem(t + d, ntp)
        peer_copy(q_recv.at[peer], q_recv.at[peer], q_ss.at[d], q_rs.at[peer], peer).wait_recv()
    q_all = jnp.concatenate([q_recv[u] for u in range(ntp)], axis=0)
    q_all_lat = q_all[:, :lw].astype(BF16)
    q_all_rot = q_all[:, lw:lw + ROPE].astype(BF16)
    copies["prope"].wait()
    def row_copy(k, d):
        return pltpu.make_async_remote_copy(
            src_ref=lat_send.at[k], dst_ref=lat_recv.at[s],
            send_sem=l_ss.at[k * ntp + d], recv_sem=l_rs.at[s],
            device_id=(k * ntp + t, lax.rem(t + d, ntp)), device_id_type=MESH)

    def pass_rows():
        total = part_send[t]
        for d in range(1, ntp):
            peer = lax.rem(t + d, ntp)
            peer_copy(part_recv.at[peer], part_recv.at[peer], p_ss.at[d], p_rs.at[peer], peer).wait_recv()
            total = total + part_recv[peer]
        copies["gain"].wait()
        copies["table"].wait()
        raw = total[:, :lw]
        scale = lax.rsqrt(jnp.mean(raw * raw, axis=-1, keepdims=True) + epsilon)
        latent = raw * scale * gain[...]
        turn = total[:, lw:lw + ROPE]
        half = ROPE // 2
        swapped = jnp.concatenate([turn[:, half:], turn[:, :half]], axis=1)
        turned = turn * table[:, :ROPE] + swapped * table[:, ROPE:]
        both = jnp.concatenate([latent, turned, jnp.zeros((gp, LANES - ROPE), F32)], axis=1)
        for k in range(groups):
            block = both[k * npos:(k + 1) * npos]
            if slot > npos:
                block = jnp.concatenate([block, jnp.zeros((slot - npos, both.shape[1]), F32)], axis=0)
            lat_send[k] = block.astype(BF16)

        for k in range(groups):
            for d in range(1, ntp):
                c = row_copy(k, d)
                c.start()
                pending.append(c)

            @pl.when(k * ntp + t != s)
            def _():
                row_copy(k, 0).start()

            @pl.when(k * ntp + t == s)
            def _():
                lat_recv[s] = lat_send[k]

    high = None
    for c in range(chunks):
        if c == chunks // 8:
            pass_rows()
        cache_copies[c].wait()
        cols = slice(c * chunk, (c + 1) * chunk)
        sc = (dot(q_all_lat, cache[cols, :], 1, 1) + dot(q_all_rot, prope[:, cols], 1, 0)) * factor
        scores[:, cols] = sc
        top = jnp.max(sc, axis=1, keepdims=True)
        high = top if high is None else jnp.maximum(high, top)

    summed = None
    mass = None
    for c in range(chunks):
        cols = slice(c * chunk, (c + 1) * chunk)
        w = jnp.exp(scores[:, cols] - high)
        part = jnp.sum(w, axis=1, keepdims=True)
        mass = part if mass is None else mass + part
        o = dot(w.astype(BF16), cache[cols, :], 1, 0)
        summed = o if summed is None else summed + o
    stats_lane = lax.broadcasted_iota(jnp.int32, (summed.shape[0], LANES), 1)
    stats = jnp.where(stats_lane < LANES // 2, high, mass)
    partial = jnp.concatenate([summed, stats], axis=1)
    for u in range(ntp):
        a_send[u] = partial[u * heads:(u + 1) * heads]
    for d in range(1, ntp):
        peer = lax.rem(t + d, ntp)
        c = peer_copy(a_send.at[peer], a_recv.at[t], a_ss.at[d], a_rs.at[t], peer)
        c.start()
        pending.append(c)

    for src in range(nsp):
        def arrive(src=src):
            pltpu.make_async_remote_copy(
                src_ref=lat_send.at[0], dst_ref=lat_recv.at[src],
                send_sem=l_ss.at[0], recv_sem=l_rs.at[src],
                device_id=(src, from_t), device_id_type=MESH).wait_recv()

        pl.when(jnp.logical_or(src != s, jnp.logical_not(self_row)))(arrive)
    copies["sel"].wait()
    copies["vu"].wait()
    arrived = lat_recv[...].reshape(nsp * slot, lw + LANES)
    block_lat = dot(sel[...], arrived[:, :lw], 1, 0).astype(BF16)
    new_turn = dot(arrived[:, lw:], sel[...], 0, 1)[:ROPE].astype(BF16)
    new_k = dot(block_lat, ku[...], 1, 0).astype(BF16)
    new_v = dot(block_lat, vu[...], 1, 0).astype(BF16)
    keys_v[...] = new_k
    vals_v[...] = new_v
    rope_v[...] = new_turn

    new_scores = (dot(q_bd, new_k, 1, 1) + dot(q_rot[:, :ROPE].astype(BF16), new_turn, 1, 0)) * factor
    peak = jnp.max(new_scores, axis=1, keepdims=True)
    own = a_send[t]
    for d in range(1, ntp):
        peer = lax.rem(t + d, ntp)
        peer_copy(a_recv.at[peer], a_recv.at[peer], a_ss.at[d], a_rs.at[peer], peer).wait_recv()
    parts = [own] + [a_recv[lax.rem(t + d, ntp)] for d in range(1, ntp)]
    for p in parts:
        peak = jnp.maximum(peak, p[:, lw:lw + 1])
    new_w = jnp.exp(new_scores - peak)
    denom = jnp.sum(new_w, axis=1, keepdims=True)
    past = None
    for p in parts:
        share = jnp.exp(p[:, lw:lw + 1] - peak)
        denom = denom + p[:, lw + LANES // 2:lw + LANES // 2 + 1] * share
        o = p[:, :lw] * share
        past = o if past is None else past + o
    out = dot(past.astype(BF16), vu[...], 1, 0) + dot(new_w.astype(BF16), new_v, 1, 0)
    out = out / denom
    att_v[...] = jnp.sum(
        jnp.where(head_mask(out.shape, VALUE_WIDTH), out, 0.0), axis=0, keepdims=True).astype(BF16)

    for c in pending:
        c.wait_send()
    for k in range(groups):
        @pl.when(k * ntp + t != s)
        def _():
            row_copy(k, 0).wait_send()


def put_out(*refs):
    sem = refs[-1]
    count = (len(refs) - 1) // 2
    copies = [pltpu.make_async_copy(refs[i], refs[count + i], sem.at[i]) for i in range(count)]
    for c in copies:
        c.start()
    for c in copies:
        c.wait()


def solution(mesh):
    nsp, ntp = mesh.shape["sp"], mesh.shape["tp"]

    def on_device(tokens, wd, wr, gain, ku, vu, cached, prope, qn, qr):
        prompts, npos, feat = tokens.shape
        owned, past, lw = cached.shape
        assert owned == 1 and prompts == nsp and prompts % ntp == 0
        turn = wr.shape[1]
        hk, hv = ku.shape[1], vu.shape[1]
        heads = qn.shape[1] // PLAIN_KEY_WIDTH
        groups = prompts // ntp
        gp = up_to(groups * npos, 8)
        slot = up_to(npos, 16)
        fresh = nsp * npos
        chunk = min(past, 1024)
        chunks = past // chunk
        width = lw + LANES

        perm = np.zeros((ntp * gp, prompts * npos), np.float32)
        table = np.zeros((nsp, gp, 2 * turn), np.float32)
        half = turn // 2
        freq = rope_theta ** (-np.arange(half) / half)
        for k in range(groups):
            for j in range(npos):
                i = k * npos + j
                for u in range(ntp):
                    perm[u * gp + i, j * prompts + k * ntp + u] = 1
                for sp in range(nsp):
                    a = (PAST_POSITIONS + sp * npos + j) * freq
                    table[sp, i] = np.concatenate([np.cos(a), np.cos(a), -np.sin(a), np.sin(a)])
        sel = np.zeros((fresh, nsp * slot), np.float32)
        for sp in range(nsp):
            for j in range(npos):
                sel[sp * npos + j, sp * slot + j] = 1
        fold = np.zeros((heads * turn, LANES), np.float32)
        fold[np.arange(heads * turn), np.arange(heads * turn) % turn] = 1

        cfg = dict(nsp=nsp, ntp=ntp, groups=groups, npos=npos, heads=heads, chunk=chunk,
                   chunks=chunks, feat=feat, lw=lw, gp=gp, slot=slot)
        args = (
            tokens.transpose(1, 0, 2).reshape(npos * prompts, feat),
            wd, wr.T, gain.reshape(1, lw), ku, vu,
            cached.reshape(past, lw), prope.reshape(past, turn).T, qn, qr,
            jnp.asarray(perm, BF16), jnp.asarray(sel, BF16), jnp.asarray(fold, BF16),
            jnp.asarray(table),
        )
        v = pltpu.VMEM
        dma = pltpu.SemaphoreType.DMA
        scratch = [
            v(args[0].shape, BF16), v((feat, lw), BF16), v((turn, feat), BF16), v((1, lw), F32),
            v(ku.shape, BF16), v(vu.shape, BF16), v((past, lw), BF16), v((turn, past), BF16),
            v(qn.shape, BF16), v(qr.shape, BF16),
            v(perm.shape, BF16), v(sel.shape, BF16), v(fold.shape, BF16), v(table.shape[1:], F32),
            v((heads, width), F32), v((ntp, heads, width), F32),
            v((ntp, gp, width), F32), v((ntp, gp, width), F32),
            v((groups, slot, width), BF16), v((nsp, slot, width), BF16),
            v((ntp, heads, width), F32), v((ntp, heads, width), F32),
            v((ntp * heads, past), F32),
            dma((13,)), dma((chunks,)),
            dma((ntp,)), dma((ntp,)), dma((ntp,)), dma((ntp,)),
            dma((groups * ntp,)), dma((nsp,)), dma((ntp,)), dma((ntp,)),
        ]
        any_spec = pl.BlockSpec(memory_space=pl.ANY)
        shapes = ((fresh, hk), (fresh, hv), (turn, fresh), (1, hv))
        room = 66_900_000 - sum(2 * up_to(r, 16) * up_to(c, LANES) for r, c in shapes)
        made = pl.pallas_call(
            functools.partial(kernel, cfg),
            out_shape=tuple(pltpu.VMEM(shape, BF16) for shape in shapes),
            in_specs=[any_spec] * len(args),
            out_specs=(pl.BlockSpec(memory_space=pltpu.VMEM),) * 4,
            scratch_shapes=scratch,
            compiler_params=pltpu.CompilerParams(
                collective_id=0, has_side_effects=True, vmem_limit_bytes=room),
        )(*args)
        keys, vals, rope, att = pl.pallas_call(
            put_out,
            out_shape=tuple(jax.ShapeDtypeStruct(shape, BF16) for shape in shapes),
            in_specs=[pl.BlockSpec(memory_space=pltpu.VMEM)] * 4,
            out_specs=(any_spec,) * 4,
            scratch_shapes=[dma((4,))],
            compiler_params=pltpu.CompilerParams(vmem_limit_bytes=4 * 1024 * 1024),
        )(*made)
        return (
            keys.reshape(1, fresh, hk),
            vals.reshape(1, fresh, hv),
            rope.T.reshape(1, fresh, turn),
            att,
        )

    in_specs = (
        P(None, "sp", "tp"),
        P(),
        P(),
        P(),
        P(None, "tp"),
        P(None, "tp"),
        P("sp", "tp", None),
        P("sp", "tp", None),
        P("sp", "tp"),
        P("sp", "tp"),
    )
    out_specs = (P("sp", None, "tp"), P("sp", None, "tp"), P("sp", None, None), P("sp", "tp"))
    return jax.shard_map(
        on_device, mesh=mesh, in_specs=in_specs, out_specs=out_specs, check_vma=False
    )
```

```python
import functools

import jax
import jax.numpy as jnp
import numpy as np
from jax import lax
from jax.experimental import pallas as pl
from jax.experimental.pallas import tpu as pltpu
from jax.sharding import PartitionSpec as P

PLAIN_KEY_WIDTH = 128
ROPE = 64
VALUE_WIDTH = 128
PAST_POSITIONS = 32768

epsilon = 1e-06
rope_theta = 10000.0
MESH = pl.DeviceIdType.MESH
F32 = jnp.float32
BF16 = jnp.bfloat16
LANES = 128


def up_to(n, m):
    return -(-n // m) * m


def dot(a, b, ca, cb):
    return lax.dot_general(a, b, (((ca,), (cb,)), ((), ())), preferred_element_type=F32)


def head_mask(shape, width):
    row = lax.broadcasted_iota(jnp.int32, shape, 0) * width
    col = lax.broadcasted_iota(jnp.int32, shape, 1)
    return (col >= row) & (col < row + width)


def kernel(cfg, *refs):
    (tok_h, wd_h, wr_h, gain_h, ku_h, vu_h, cache_h, prope_h, qn_h, qr_h,
     perm_h, sel_h, fold_h, table_h,
     keys_v, vals_v, rope_v, att_v,
     tok, wd, wr, gain, ku, vu, cache, prope, qn, qr, perm, sel, fold, table,
     q_send, q_recv, part_send, part_recv, lat_send, lat_recv, a_send, a_recv, scores,
     load_sem, cache_sem,
     q_ss, q_rs, p_ss, p_rs, l_ss, l_rs, a_ss, a_rs) = refs
    nsp, ntp, groups, npos, heads, chunk, chunks = (
        cfg[k] for k in ("nsp", "ntp", "groups", "npos", "heads", "chunk", "chunks"))
    feat, lw, gp, slot = cfg["feat"], cfg["lw"], cfg["gp"], cfg["slot"]
    s = lax.axis_index("sp")
    t = lax.axis_index("tp")
    factor = (PLAIN_KEY_WIDTH + ROPE) ** (-0.5)

    copies = {}

    def load(name, src, dst):
        c = pltpu.make_async_copy(src, dst, load_sem.at[len(copies)])
        c.start()
        copies[name] = c

    rows0 = pl.multiple_of(t * feat, LANES)
    load("qn", qn_h, qn)
    load("qr", qr_h, qr)
    load("ku", ku_h, ku)
    load("fold", fold_h, fold)
    load("tok", tok_h, tok)
    load("perm", perm_h, perm)
    load("wd", wd_h.at[pl.ds(rows0, feat), :], wd)
    load("wr", wr_h.at[:, pl.ds(rows0, feat)], wr)
    load("gain", gain_h, gain)
    load("table", table_h.at[s], table)
    load("sel", sel_h, sel)

    barrier = pltpu.get_barrier_semaphore()
    for d in range(1, ntp):
        pl.semaphore_signal(barrier, inc=1, device_id=(s, lax.rem(t + d, ntp)), device_id_type=MESH)
    from_t = lax.rem(s, ntp)
    for src in range(nsp):
        @pl.when(src != s)
        def _():
            pl.semaphore_signal(barrier, inc=1, device_id=(src, from_t), device_id_type=MESH)

    for name in ("qn", "qr", "ku", "fold", "tok", "perm", "wd", "wr"):
        copies[name].wait()
    load("prope", prope_h, prope)
    cache_copies = []
    for c in range(chunks):
        cc = pltpu.make_async_copy(
            cache_h.at[pl.ds(c * chunk, chunk), :], cache.at[pl.ds(c * chunk, chunk), :], cache_sem.at[c])
        cc.start()
        cache_copies.append(cc)
    load("vu", vu_h, vu)
    qn_row = jnp.broadcast_to(qn[...].astype(F32), (heads, qn.shape[1]))
    q_bd = jnp.where(head_mask(qn_row.shape, PLAIN_KEY_WIDTH), qn_row, 0.0).astype(BF16)
    qr_row = jnp.broadcast_to(qr[...].astype(F32), (heads, qr.shape[1]))
    qr_bd = jnp.where(head_mask(qr_row.shape, ROPE), qr_row, 0.0).astype(BF16)
    q_lat = dot(q_bd, ku[...], 1, 1).astype(BF16).astype(F32)
    q_rot = dot(qr_bd, fold[...], 1, 0)
    q_own = jnp.concatenate([q_lat, q_rot], axis=1)
    q_send[...] = q_own
    q_recv[t] = q_own

    self_row = from_t == t
    pl.semaphore_wait(
        barrier, ntp - 1 + ntp * groups - ntp * jnp.where(self_row, 1, 0).astype(jnp.int32))

    def peer_copy(src, dst, ssem, rsem, peer):
        return pltpu.make_async_remote_copy(
            src_ref=src, dst_ref=dst, send_sem=ssem, recv_sem=rsem,
            device_id=(s, peer), device_id_type=MESH)

    pending = []
    for d in range(1, ntp):
        c = peer_copy(q_send, q_recv.at[t], q_ss.at[d], q_rs.at[t], lax.rem(t + d, ntp))
        c.start()
        pending.append(c)

    rows = dot(perm[...], tok[...], 1, 0).astype(BF16)
    lat_part = dot(rows, wd[...], 1, 0)
    rope_part = dot(rows, wr[...], 1, 1)
    for u in range(ntp):
        part_send[u, :, :lw] = lat_part[u * gp:(u + 1) * gp]
        part_send[u, :, lw:lw + ROPE] = rope_part[u * gp:(u + 1) * gp]
        part_send[u, :, lw + ROPE:] = jnp.zeros((gp, LANES - ROPE), F32)
    for d in range(1, ntp):
        peer = lax.rem(t + d, ntp)
        c = peer_copy(part_send.at[peer], part_recv.at[t], p_ss.at[d], p_rs.at[t], peer)
        c.start()
        pending.append(c)

    for d in range(1, ntp):
        peer = lax.rem(t + d, ntp)
        peer_copy(q_recv.at[peer], q_recv.at[peer], q_ss.at[d], q_rs.at[peer], peer).wait_recv()
    q_all = jnp.concatenate([q_recv[u] for u in range(ntp)], axis=0)
    q_all_lat = q_all[:, :lw].astype(BF16)
    q_all_rot = q_all[:, lw:lw + ROPE].astype(BF16)
    copies["prope"].wait()
    def row_copy(k, d):
        return pltpu.make_async_remote_copy(
            src_ref=lat_send.at[k], dst_ref=lat_recv.at[s],
            send_sem=l_ss.at[k * ntp + d], recv_sem=l_rs.at[s],
            device_id=(k * ntp + t, lax.rem(t + d, ntp)), device_id_type=MESH)

    def pass_rows():
        total = part_send[t]
        for d in range(1, ntp):
            peer = lax.rem(t + d, ntp)
            peer_copy(part_recv.at[peer], part_recv.at[peer], p_ss.at[d], p_rs.at[peer], peer).wait_recv()
            total = total + part_recv[peer]
        copies["gain"].wait()
        copies["table"].wait()
        raw = total[:, :lw]
        scale = lax.rsqrt(jnp.mean(raw * raw, axis=-1, keepdims=True) + epsilon)
        latent = raw * scale * gain[...]
        turn = total[:, lw:lw + ROPE]
        half = ROPE // 2
        swapped = jnp.concatenate([turn[:, half:], turn[:, :half]], axis=1)
        turned = turn * table[:, :ROPE] + swapped * table[:, ROPE:]
        both = jnp.concatenate([latent, turned, jnp.zeros((gp, LANES - ROPE), F32)], axis=1)
        for k in range(groups):
            block = both[k * npos:(k + 1) * npos]
            if slot > npos:
                block = jnp.concatenate([block, jnp.zeros((slot - npos, both.shape[1]), F32)], axis=0)
            lat_send[k] = block.astype(BF16)

        for k in range(groups):
            for d in range(1, ntp):
                c = row_copy(k, d)
                c.start()
                pending.append(c)

            @pl.when(k * ntp + t != s)
            def _():
                row_copy(k, 0).start()

            @pl.when(k * ntp + t == s)
            def _():
                lat_recv[s] = lat_send[k]

    high = None
    for c in range(chunks):
        if c == chunks // 4:
            pass_rows()
        cache_copies[c].wait()
        cols = slice(c * chunk, (c + 1) * chunk)
        sc = (dot(q_all_lat, cache[cols, :], 1, 1) + dot(q_all_rot, prope[:, cols], 1, 0)) * factor
        scores[:, cols] = sc
        top = jnp.max(sc, axis=1, keepdims=True)
        high = top if high is None else jnp.maximum(high, top)

    summed = None
    mass = None
    for c in range(chunks):
        cols = slice(c * chunk, (c + 1) * chunk)
        w = jnp.exp(scores[:, cols] - high)
        part = jnp.sum(w, axis=1, keepdims=True)
        mass = part if mass is None else mass + part
        o = dot(w.astype(BF16), cache[cols, :], 1, 0)
        summed = o if summed is None else summed + o
    stats_lane = lax.broadcasted_iota(jnp.int32, (summed.shape[0], LANES), 1)
    stats = jnp.where(stats_lane < LANES // 2, high, mass)
    partial = jnp.concatenate([summed, stats], axis=1)
    for u in range(ntp):
        a_send[u] = partial[u * heads:(u + 1) * heads]
    for d in range(1, ntp):
        peer = lax.rem(t + d, ntp)
        c = peer_copy(a_send.at[peer], a_recv.at[t], a_ss.at[d], a_rs.at[t], peer)
        c.start()
        pending.append(c)

    for src in range(nsp):
        def arrive(src=src):
            pltpu.make_async_remote_copy(
                src_ref=lat_send.at[0], dst_ref=lat_recv.at[src],
                send_sem=l_ss.at[0], recv_sem=l_rs.at[src],
                device_id=(src, from_t), device_id_type=MESH).wait_recv()

        pl.when(jnp.logical_or(src != s, jnp.logical_not(self_row)))(arrive)
    copies["sel"].wait()
    copies["vu"].wait()
    arrived = lat_recv[...].reshape(nsp * slot, lw + LANES)
    block_lat = dot(sel[...], arrived[:, :lw], 1, 0).astype(BF16)
    new_turn = dot(arrived[:, lw:], sel[...], 0, 1)[:ROPE].astype(BF16)
    new_k = dot(block_lat, ku[...], 1, 0).astype(BF16)
    new_v = dot(block_lat, vu[...], 1, 0).astype(BF16)
    keys_v[...] = new_k
    vals_v[...] = new_v
    rope_v[...] = new_turn

    new_scores = (dot(q_bd, new_k, 1, 1) + dot(q_rot[:, :ROPE].astype(BF16), new_turn, 1, 0)) * factor
    peak = jnp.max(new_scores, axis=1, keepdims=True)
    own = a_send[t]
    for d in range(1, ntp):
        peer = lax.rem(t + d, ntp)
        peer_copy(a_recv.at[peer], a_recv.at[peer], a_ss.at[d], a_rs.at[peer], peer).wait_recv()
    parts = [own] + [a_recv[lax.rem(t + d, ntp)] for d in range(1, ntp)]
    for p in parts:
        peak = jnp.maximum(peak, p[:, lw:lw + 1])
    new_w = jnp.exp(new_scores - peak)
    denom = jnp.sum(new_w, axis=1, keepdims=True)
    past = None
    for p in parts:
        share = jnp.exp(p[:, lw:lw + 1] - peak)
        denom = denom + p[:, lw + LANES // 2:lw + LANES // 2 + 1] * share
        o = p[:, :lw] * share
        past = o if past is None else past + o
    out = dot(past.astype(BF16), vu[...], 1, 0) + dot(new_w.astype(BF16), new_v, 1, 0)
    out = out / denom
    att_v[...] = jnp.sum(
        jnp.where(head_mask(out.shape, VALUE_WIDTH), out, 0.0), axis=0, keepdims=True).astype(BF16)

    for c in pending:
        c.wait_send()
    for k in range(groups):
        @pl.when(k * ntp + t != s)
        def _():
            row_copy(k, 0).wait_send()


def put_out(*refs):
    sem = refs[-1]
    count = (len(refs) - 1) // 2
    copies = [pltpu.make_async_copy(refs[i], refs[count + i], sem.at[i]) for i in range(count)]
    for c in copies:
        c.start()
    for c in copies:
        c.wait()


def solution(mesh):
    nsp, ntp = mesh.shape["sp"], mesh.shape["tp"]

    def on_device(tokens, wd, wr, gain, ku, vu, cached, prope, qn, qr):
        prompts, npos, feat = tokens.shape
        owned, past, lw = cached.shape
        assert owned == 1 and prompts == nsp and prompts % ntp == 0
        turn = wr.shape[1]
        hk, hv = ku.shape[1], vu.shape[1]
        heads = qn.shape[1] // PLAIN_KEY_WIDTH
        groups = prompts // ntp
        gp = up_to(groups * npos, 8)
        slot = up_to(npos, 16)
        fresh = nsp * npos
        chunk = min(past, 1024)
        chunks = past // chunk
        width = lw + LANES

        perm = np.zeros((ntp * gp, prompts * npos), np.float32)
        table = np.zeros((nsp, gp, 2 * turn), np.float32)
        half = turn // 2
        freq = rope_theta ** (-np.arange(half) / half)
        for k in range(groups):
            for j in range(npos):
                i = k * npos + j
                for u in range(ntp):
                    perm[u * gp + i, j * prompts + k * ntp + u] = 1
                for sp in range(nsp):
                    a = (PAST_POSITIONS + sp * npos + j) * freq
                    table[sp, i] = np.concatenate([np.cos(a), np.cos(a), -np.sin(a), np.sin(a)])
        sel = np.zeros((fresh, nsp * slot), np.float32)
        for sp in range(nsp):
            for j in range(npos):
                sel[sp * npos + j, sp * slot + j] = 1
        fold = np.zeros((heads * turn, LANES), np.float32)
        fold[np.arange(heads * turn), np.arange(heads * turn) % turn] = 1

        cfg = dict(nsp=nsp, ntp=ntp, groups=groups, npos=npos, heads=heads, chunk=chunk,
                   chunks=chunks, feat=feat, lw=lw, gp=gp, slot=slot)
        args = (
            tokens.transpose(1, 0, 2).reshape(npos * prompts, feat),
            wd, wr.T, gain.reshape(1, lw), ku, vu,
            cached.reshape(past, lw), prope.reshape(past, turn).T, qn, qr,
            jnp.asarray(perm, BF16), jnp.asarray(sel, BF16), jnp.asarray(fold, BF16),
            jnp.asarray(table),
        )
        v = pltpu.VMEM
        dma = pltpu.SemaphoreType.DMA
        scratch = [
            v(args[0].shape, BF16), v((feat, lw), BF16), v((turn, feat), BF16), v((1, lw), F32),
            v(ku.shape, BF16), v(vu.shape, BF16), v((past, lw), BF16), v((turn, past), BF16),
            v(qn.shape, BF16), v(qr.shape, BF16),
            v(perm.shape, BF16), v(sel.shape, BF16), v(fold.shape, BF16), v(table.shape[1:], F32),
            v((heads, width), F32), v((ntp, heads, width), F32),
            v((ntp, gp, width), F32), v((ntp, gp, width), F32),
            v((groups, slot, width), BF16), v((nsp, slot, width), BF16),
            v((ntp, heads, width), F32), v((ntp, heads, width), F32),
            v((ntp * heads, past), F32),
            dma((13,)), dma((chunks,)),
            dma((ntp,)), dma((ntp,)), dma((ntp,)), dma((ntp,)),
            dma((groups * ntp,)), dma((nsp,)), dma((ntp,)), dma((ntp,)),
        ]
        any_spec = pl.BlockSpec(memory_space=pl.ANY)
        shapes = ((fresh, hk), (fresh, hv), (turn, fresh), (1, hv))
        room = 66_900_000 - sum(2 * up_to(r, 16) * up_to(c, LANES) for r, c in shapes)
        made = pl.pallas_call(
            functools.partial(kernel, cfg),
            out_shape=tuple(pltpu.VMEM(shape, BF16) for shape in shapes),
            in_specs=[any_spec] * len(args),
            out_specs=(pl.BlockSpec(memory_space=pltpu.VMEM),) * 4,
            scratch_shapes=scratch,
            compiler_params=pltpu.CompilerParams(
                collective_id=0, has_side_effects=True, vmem_limit_bytes=room),
        )(*args)
        keys, vals, rope, att = pl.pallas_call(
            put_out,
            out_shape=tuple(jax.ShapeDtypeStruct(shape, BF16) for shape in shapes),
            in_specs=[pl.BlockSpec(memory_space=pltpu.VMEM)] * 4,
            out_specs=(any_spec,) * 4,
            scratch_shapes=[dma((4,))],
            compiler_params=pltpu.CompilerParams(vmem_limit_bytes=4 * 1024 * 1024),
        )(*made)
        return (
            keys.reshape(1, fresh, hk),
            vals.reshape(1, fresh, hv),
            rope.T.reshape(1, fresh, turn),
            att,
        )

    in_specs = (
        P(None, "sp", "tp"),
        P(),
        P(),
        P(),
        P(None, "tp"),
        P(None, "tp"),
        P("sp", "tp", None),
        P("sp", "tp", None),
        P("sp", "tp"),
        P("sp", "tp"),
    )
    out_specs = (P("sp", None, "tp"), P("sp", None, "tp"), P("sp", None, None), P("sp", "tp"))
    return jax.shard_map(
        on_device, mesh=mesh, in_specs=in_specs, out_specs=out_specs, check_vma=False
    )
```
